256 devices in a mesh: ep: 64 (over z, x, core), tp: 4 (over y).
Axes of the slice: x: 4, y: 4, z: 8, core: 2. Of those that a mesh axis runs over, the one named last changes fastest.
Arguments:
- query_rows: bfloat16 [16384, 1024], P('ep', 'tp'), may hold values from -8 to 8
- key_rows: bfloat16 [16384, 256], P('ep', 'tp'), may hold values from -8 to 8
- value_rows: bfloat16 [16384, 256], P('ep', 'tp'), may hold values from -16 to 16
- query_gain: float32 [64], replicated, may hold values from 0.5 to 7.5
- key_gain: float32 [64], replicated, may hold values from 0.5 to 7.5
- moe_tokens: bfloat16 [32768, 2048], P(('ep', 'tp')), may hold values from -6 to 6
- norm_gain: float32 [2048], replicated, may hold values from 0.1 to 1.9
- routes: int32 [32768, 2], P('ep'), may hold values from 0 to 63, all different within a row; in each aligned block of 128 rows (0 to 127, 128 to 255, ...) at most 8 rows name the same one
- route_weights: float32 [32768, 2], P('ep'), may hold values from 0.1 to 1
- expert_gate: bfloat16 [64, 2048, 1024], P('ep', None, 'tp'), may hold values from -0.125 to 0.125
- expert_up: bfloat16 [64, 2048, 1024], P('ep', None, 'tp'), may hold values from -0.125 to 0.125
- expert_down: bfloat16 [64, 1024, 2048], P('ep', 'tp'), may hold values from -0.1875 to 0.1875
- shared_gate: bfloat16 [2048, 1024], P(None, 'tp'), may hold values from -0.125 to 0.125
- shared_up: bfloat16 [2048, 1024], P(None, 'tp'), may hold values from -0.125 to 0.125
- shared_down: bfloat16 [1024, 2048], P('tp'), may hold values from -0.1875 to 0.1875
Outputs:
- attn_out: bfloat16 [16384, 1024], P('ep', 'tp')
- moe_out: bfloat16 [32768, 2048], P(('ep', 'tp'))
The draws below stay inside these ranges and needn't reach their ends.
Inputs may be any that keep to these rules, and one draw needn't show every extreme that they name: `routes`: each row names 2 different experts. Within each aligned block of 128 rows no expert is named more than 8 times, and in every draw some expert is named exactly 8 times in some block.
All inputs are finite; a program needn't handle non-finite values.
Results may differ from the reference program's by a relative error of at most 0.012.
The reference program's roundings to bfloat16 on the way count: a program that leaves them out, or rounds other values in their place, can miss the bound.
Values may be sent and summed in bfloat16 or wider, within the bound.
A program may use at most 192 MiB of HBM per device.

```python
import math
import jax
import jax.numpy as jnp
import numpy as np
from jax import lax

D = 2048
HEADS = 16
KV_HEADS = 4
HD = 64
F = 1024
TOP = 2
GRID_W = 64
TOK_B = 128
TOKENS_A = 16384
TOKENS_B = 32768
EXPERTS = 64
CAP = 8
N_TP = 4


def draw_key_rows(key, part):
    result = jnp.clip(jax.random.normal(jax.random.fold_in(key, 72), (TOKENS_A, KV_HEADS * HD), jnp.float32), -6.0, 6.0)
    return result.astype(jnp.bfloat16)


def draw_query_rows(key, part):
    result = jnp.clip(jax.random.normal(jax.random.fold_in(key, 73), (TOKENS_A, HEADS * HD), jnp.float32), -6.0, 6.0)
    return result.astype(jnp.bfloat16)


def gain_draw(key, salt):
    result = jax.random.uniform(jax.random.fold_in(key, salt + 3), (HD,), jnp.float32, 1.2, 1.8)
    return result


def draw_query_gain(key, part):
    return gain_draw(key, 80)


def draw_key_gain(key, part):
    return gain_draw(key, 90)


def level_of(key, dims, pieces, low, top_value):
    factor_of, own = 1.0, jax.random.fold_in(key, 6)
    for axis_at, blocks in pieces:
        heights = jnp.exp(jax.random.uniform(jax.random.fold_in(own, axis_at), (blocks,), jnp.float32, low / len(pieces), top_value / len(pieces)))
        factor_of = factor_of * jnp.repeat(heights, dims[axis_at] // blocks).reshape([-1 if axis == axis_at else 1 for axis in range(len(dims))])
    return factor_of


def assign_block(stream_key, own, number, rows, amount, top, bound, slope):
    ranking = jax.random.permutation(stream_key, amount)
    crowded, common = portions_of(amount, rows * top, bound, slope, True), portions_of(amount, rows * top, bound, slope, False)
    places = jnp.arange(amount)

    def named(sizes, rotation):
        used = int((sizes > 0).sum())
        fixed = max(1, used // 4)
        passed = fixed + (places - fixed + rotation * (used - fixed)) % max(1, amount - fixed)
        return jnp.zeros((amount,), jnp.int32).at[ranking[jnp.where(places < fixed, places, passed)]].set(jnp.asarray(sizes, jnp.int32))

    sizes = jnp.where(number % 4 == 0, named(crowded, number // 4), named(common, number - number // 4 - 1))
    mixed = jax.random.permutation(jax.random.fold_in(own, 3), amount)
    source_of, receiver = mixed[0:amount // 2 * 2:2], mixed[1:amount // 2 * 2:2]
    room = jnp.minimum(sizes[source_of] - 1, bound - sizes[receiver]) // 2
    room = jnp.where((source_of == ranking[0]) | (receiver == ranking[0]) | (sizes[receiver] == 0), 0, jnp.maximum(room, 0))
    passed = jax.random.randint(jax.random.fold_in(own, 4), (amount // 2,), 0, 1 << 20) % (room + 1)
    sizes = sizes.at[source_of].add(-passed).at[receiver].add(passed)
    items = jnp.searchsorted(jnp.cumsum(sizes), jnp.arange(rows * top), side="right").astype(jnp.int32)
    table = items.reshape(top, rows).T
    table = table[jax.random.permutation(jax.random.fold_in(own, 1), rows)]
    rotation = jax.random.randint(jax.random.fold_in(own, 2), (rows, 1), 0, top)
    return jnp.take_along_axis(table, (jnp.arange(top)[None, :] + rotation) % top, axis=1)


def portions_of(number_of, total, limit, skew, full):
    weights = [(1 << 20) // math.isqrt(standing ** skew) + 1 for standing in range(1, number_of + 1)]
    largest = limit if full else min(limit, max(-(-total // number_of), total * weights[0] // sum(weights)))
    least = 1 if total - largest >= number_of - 1 else 0
    holding, surplus = [largest] + [least] * (number_of - 1), total - largest - least * (number_of - 1)
    while surplus > 0:
        movable = [i for i in range(1, number_of) if holding[i] < largest] or [i for i in range(1, number_of) if holding[i] < limit]
        pool, remaining = sum([weights[i] for i in movable]), surplus
        for i in movable:
            more = min(limit - holding[i], max(1, remaining * weights[i] // pool), surplus)
            holding[i] = holding[i] + more
            surplus = surplus - more
    return np.array(holding)


def gaussian(key, extent, width, reach, pieces=(), kind=jnp.bfloat16):
    entries = width * jax.random.normal(key, extent, jnp.float32)
    if pieces:
        entries = entries * level_of(key, extent, pieces, -0.22, 0.18)
    return jnp.clip(entries, -reach, reach).astype(kind)


def setup_inputs(seed: int = 0) -> dict:
    key_list = jax.random.split(jax.random.key(seed), 16)
    query_rows = draw_query_rows(jax.random.fold_in(key_list[15], 71), 0)
    key_rows = draw_key_rows(jax.random.fold_in(key_list[15], 71), 0)
    value_rows = gaussian(key_list[2], (TOKENS_A, KV_HEADS * HD), 3.0, 16.0, ((0, 64), (1, 4)))
    query_gain = draw_query_gain(jax.random.fold_in(key_list[15], 71), 0)
    key_gain = draw_key_gain(jax.random.fold_in(key_list[15], 71), 0)
    moe_tokens = gaussian(key_list[5], (TOKENS_B, D), 1.0, 6.0, ((0, 256),))
    norm_gain = jnp.clip(1.0 + 0.18 * jax.random.normal(key_list[6], (D,), jnp.float32), 0.1, 1.9)
    routes_keys = jax.random.split(jax.random.fold_in(key_list[7], 1), TOKENS_B // TOK_B)
    routes_turns = jax.random.permutation(jax.random.fold_in(key_list[7], 3), TOKENS_B // TOK_B)
    routes = jax.vmap(lambda own, number: assign_block(jax.random.fold_in(key_list[7], 2), own, number, TOK_B, EXPERTS, TOP, CAP, 1))(routes_keys, routes_turns).reshape((TOKENS_B, TOP))
    route_weights = jnp.clip(0.1 + 0.9 * jax.random.uniform(key_list[8], (TOKENS_B, TOP), jnp.float32) ** level_of(key_list[8], (TOKENS_B, TOP), ((0, 64),), -0.2, 0.2), 0.1, 1.0)
    expert_gate = gaussian(key_list[9], (EXPERTS, D, F), D ** -0.5, 0.125, ((0, 64), (2, 4)))
    expert_up = gaussian(key_list[10], (EXPERTS, D, F), D ** -0.5, 0.125, ((0, 64), (2, 4)))
    expert_down = gaussian(key_list[11], (EXPERTS, F, D), F ** -0.5, 0.1875, ((0, 64), (1, 4)))
    shared_gate = gaussian(key_list[12], (D, F), D ** -0.5, 0.125, ((1, 4),))
    shared_up = gaussian(key_list[13], (D, F), D ** -0.5, 0.125, ((1, 4),))
    shared_down = gaussian(key_list[14], (F, D), F ** -0.5, 0.1875, ((0, 4),))
    return {"query_rows": query_rows, "key_rows": key_rows, "value_rows": value_rows, "query_gain": query_gain, "key_gain": key_gain, "moe_tokens": moe_tokens, "norm_gain": norm_gain, "routes": routes, "route_weights": route_weights, "expert_gate": expert_gate, "expert_up": expert_up, "expert_down": expert_down, "shared_gate": shared_gate, "shared_up": shared_up, "shared_down": shared_down}


epsilon = 1e-06
rotary_base = 10000.0
routed_scale = 2.5

def rotate_heads(heads_in, gain_row, positions):
    values32 = heads_in.astype(jnp.float32)
    scaled = values32 * lax.rsqrt(lax.optimization_barrier(jnp.mean(values32 * values32, axis=-1, keepdims=True)) + epsilon) * gain_row
    pair_count = scaled.shape[-1] // 4
    inv_freq = rotary_base ** (-jnp.arange(pair_count, dtype=jnp.float32) / pair_count)
    grid_row = (positions // GRID_W).astype(jnp.float32)
    grid_col = (positions % GRID_W).astype(jnp.float32)
    angles = jnp.concatenate([grid_row[:, None] * inv_freq, grid_col[:, None] * inv_freq], axis=-1)[:, None, :]
    cosine = jnp.cos(angles)
    sine_part = jnp.sin(angles)
    first_half = scaled[..., 0::2]
    second_half = scaled[..., 1::2]
    turned = jnp.stack([first_half * cosine - second_half * sine_part, first_half * sine_part + second_half * cosine], axis=-1)
    return turned.reshape(scaled.shape).astype(jnp.bfloat16)

def attention(query_rows, key_rows, value_rows, query_gain, key_gain):
    token_count = query_rows.shape[0]
    group = HEADS // KV_HEADS
    positions = jnp.arange(token_count, dtype=jnp.int32)
    q_rot = rotate_heads(query_rows.reshape(token_count, HEADS, HD), query_gain, positions)
    k_rot = rotate_heads(key_rows.reshape(token_count, KV_HEADS, HD), key_gain, positions)
    keys32 = lax.optimization_barrier(k_rot).astype(jnp.float32)
    values32 = value_rows.reshape(token_count, KV_HEADS, HD).astype(jnp.float32)
    block_len = math.gcd(token_count, 256)
    q_blocks = lax.optimization_barrier(q_rot).reshape(token_count // block_len, block_len, KV_HEADS, group, HD)

    def one_block(q_block):
        scores = jnp.einsum('qgrd,sgd->qgrs', q_block.astype(jnp.float32), keys32) * HD ** (-0.5)
        row_max = lax.optimization_barrier(jnp.max(scores, axis=-1, keepdims=True))
        weights = jnp.exp(scores - row_max)
        row_sum = lax.optimization_barrier(jnp.sum(weights, axis=-1, keepdims=True))
        rounded = lax.optimization_barrier(weights.astype(jnp.bfloat16)).astype(jnp.float32)
        mixed = jnp.einsum('qgrs,sgd->qgrd', rounded, values32)
        return (mixed / row_sum).astype(jnp.bfloat16)
    result = lax.map(one_block, q_blocks)
    return result.reshape(token_count, HEADS * HD)

def feed_forward(rows_in, w_gate, w_up, w_down):
    gate_proj = jnp.dot(rows_in, w_gate, preferred_element_type=jnp.float32)
    up_proj = jnp.dot(rows_in, w_up, preferred_element_type=jnp.float32)
    hidden = lax.optimization_barrier((jax.nn.silu(gate_proj) * up_proj).astype(jnp.bfloat16))
    block_width = hidden.shape[-1] // N_TP
    summed = jnp.zeros((rows_in.shape[0], w_down.shape[1]), jnp.float32)
    for part_index in range(N_TP):
        lower = part_index * block_width
        partial_sum = jnp.dot(hidden[:, lower:lower + block_width], w_down[lower:lower + block_width], preferred_element_type=jnp.float32).astype(jnp.bfloat16)
        summed = summed + lax.optimization_barrier(partial_sum).astype(jnp.float32)
    return summed

def mixture(moe_tokens, norm_gain, routes, route_weights, expert_gate, expert_up, expert_down, shared_gate, shared_up, shared_down):
    total_rows = moe_tokens.shape[0]
    blocks = total_rows // TOK_B
    values32 = moe_tokens.astype(jnp.float32)
    normed = (values32 * lax.rsqrt(lax.optimization_barrier(jnp.mean(values32 * values32, axis=-1, keepdims=True)) + epsilon) * norm_gain).astype(jnp.bfloat16)
    normed = lax.optimization_barrier(normed)
    gates = route_weights / lax.optimization_barrier(jnp.sum(route_weights, axis=-1, keepdims=True)) * routed_scale
    chosen = routes.reshape(blocks, TOK_B * TOP).astype(jnp.int32)
    one_hot = (chosen[:, :, None] == jnp.arange(EXPERTS, dtype=jnp.int32)[None, None, :]).astype(jnp.int32)
    ranks = lax.optimization_barrier(jnp.sum((jnp.cumsum(one_hot, axis=1) - one_hot) * one_hot, axis=2))
    block_ids = jnp.arange(blocks, dtype=jnp.int32)[:, None]
    dest = (chosen * blocks + block_ids) * CAP + ranks
    rows_from = block_ids * TOK_B + jnp.arange(TOK_B * TOP, dtype=jnp.int32)[None, :] // TOP
    slot_rows = jnp.full((EXPERTS * blocks * CAP,), total_rows, jnp.int32).at[dest.reshape(-1)].set(rows_from.reshape(-1))
    padded = jnp.concatenate([normed, jnp.zeros((1, D), jnp.bfloat16)], axis=0)

    def one_expert(inputs):
        index_rows, w_gate, w_up, w_down = inputs
        return feed_forward(padded[index_rows], w_gate, w_up, w_down).astype(jnp.bfloat16)
    expert_rows = lax.map(one_expert, (slot_rows.reshape(EXPERTS, blocks * CAP), expert_gate, expert_up, expert_down))
    flat_rows = lax.optimization_barrier(expert_rows.reshape(EXPERTS * blocks * CAP, D))
    picked = flat_rows[dest.reshape(-1)].astype(jnp.float32).reshape(total_rows, TOP, D)
    routed = lax.optimization_barrier(jnp.sum(gates[:, :, None] * picked, axis=1))
    shared = feed_forward(normed, shared_gate, shared_up, shared_down)
    return (routed + shared).astype(jnp.bfloat16)

def reference(query_rows, key_rows, value_rows, query_gain, key_gain, moe_tokens, norm_gain, routes, route_weights, expert_gate, expert_up, expert_down, shared_gate, shared_up, shared_down):
    attn_out = attention(query_rows, key_rows, value_rows, query_gain, key_gain)
    moe_out = mixture(moe_tokens, norm_gain, routes, route_weights, expert_gate, expert_up, expert_down, shared_gate, shared_up, shared_down)
    return (attn_out, moe_out)
```

```python
import jax
import jax.numpy as jnp
from jax import lax
from jax.sharding import Mesh
from jax.sharding import PartitionSpec as P

GRID_W = 64
EP = ("ep_0", "ep_1", "ep_2")
EP_TP = ("ep_0", "ep_1", "ep_2", "tp")


epsilon = 1e-06
rotary_base = 10000.0
routed_scale = 2.5


def joined_along(pieces, dim):
    lengths = list(pieces.shape[1:])
    lengths[dim] *= pieces.shape[0]
    return jnp.moveaxis(pieces, 0, dim).reshape(lengths)


def stacked_from(array, axes, order):
    pieces = array
    for k in order:
        pieces = lax.all_gather(pieces, axes[k])
    done = order[::-1]
    back = [done.index(k) for k in range(len(axes))]
    pieces = pieces.transpose(*back, *range(len(axes), pieces.ndim))
    return pieces.reshape(-1, *array.shape)


def gathered_by_axis(array, axes, order, dim):
    return joined_along(stacked_from(array, axes, order), dim)


def copy_for_each(array, axis):
    count = lax.axis_size(axis)
    return lax.all_to_all(
        jnp.broadcast_to(array[None], (count, *array.shape)), axis, 0, 0, tiled=True
    )


def gathered_copies(array, axis, dim):
    pieces = copy_for_each(array, axis)
    return joined_along(pieces, dim)


def cut_along(array, dim, count):
    before, after = (array.shape[:dim], array.shape[dim + 1 :])
    return jnp.moveaxis(array.reshape(*before, count, -1, *after), dim, 0)


def sent_and_summed(array, axis, dim):
    pieces = cut_along(array, dim, lax.axis_size(axis))
    arrived = lax.all_to_all(pieces, axis, split_axis=0, concat_axis=0, tiled=True)
    return arrived.astype(jnp.float32).sum(axis=0)


def rotate_heads(heads_in, gain_row, positions):
    values32 = heads_in.astype(jnp.float32)
    scaled = (
        values32
        * lax.rsqrt(jnp.mean(values32 * values32, axis=-1, keepdims=True) + epsilon)
        * gain_row
    )
    pair_count = scaled.shape[-1] // 4
    inv_freq = rotary_base ** (-jnp.arange(pair_count, dtype=jnp.float32) / pair_count)
    grid_row = (positions // GRID_W).astype(jnp.float32)
    grid_col = (positions % GRID_W).astype(jnp.float32)
    angles = jnp.concatenate([grid_row[:, None] * inv_freq, grid_col[:, None] * inv_freq], axis=-1)[
        :, None, :
    ]
    cosine = jnp.cos(angles)
    sine_part = jnp.sin(angles)
    first_half = scaled[..., 0::2]
    second_half = scaled[..., 1::2]
    turned = jnp.stack(
        [
            first_half * cosine - second_half * sine_part,
            first_half * sine_part + second_half * cosine,
        ],
        axis=-1,
    )
    return turned.reshape(scaled.shape).astype(jnp.bfloat16)


def span_length(row_count):
    length = min(row_count, 2048)
    while row_count % length:
        length -= 1
    return length


def attend(query_rows, key_rows, value_rows, query_gain, key_gain):
    row_count = query_rows.shape[0]
    head_size = query_gain.shape[0]
    q_heads = query_rows.shape[1] // head_size
    kv_heads = key_rows.shape[1] // head_size
    group = q_heads // kv_heads
    scale = head_size ** (-0.5)
    positions = lax.axis_index(EP) * row_count + jnp.arange(row_count, dtype=jnp.int32)
    q_rot = rotate_heads(query_rows.reshape(row_count, q_heads, head_size), query_gain, positions)
    k_rot = rotate_heads(key_rows.reshape(row_count, kv_heads, head_size), key_gain, positions)
    key_value = jnp.stack([k_rot, value_rows.reshape(row_count, kv_heads, head_size)], axis=2)
    key_value = key_value.reshape(row_count, kv_heads * 2 * head_size)
    q_grouped = q_rot.reshape(row_count, kv_heads, group, head_size).transpose(1, 2, 0, 3)
    q_grouped = q_grouped.reshape(kv_heads, group * row_count, head_size)
    query_count = group * row_count
    initial = (
        jnp.full((kv_heads, query_count), -jnp.inf, jnp.float32),
        jnp.zeros((kv_heads, query_count), jnp.float32),
        jnp.zeros((kv_heads, query_count, head_size), jnp.float32),
    )

    def one_span(carried, span_rows):
        run_max, run_sum, mixed = carried
        keys_span = span_rows[:, :, 0, :]
        values_span = span_rows[:, :, 1, :]
        scores = (
            jnp.einsum("hrd,shd->hrs", q_grouped, keys_span, preferred_element_type=jnp.float32)
            * scale
        )
        new_max = jnp.maximum(run_max, jnp.max(scores, axis=-1))
        factor = jnp.exp(run_max - new_max)
        weights = jnp.exp(scores - new_max[..., None])
        run_sum = run_sum * factor + jnp.sum(weights, axis=-1)
        added = jnp.einsum(
            "hrs,shd->hrd",
            weights.astype(jnp.bfloat16),
            values_span,
            preferred_element_type=jnp.float32,
        )
        mixed = mixed * factor[..., None] + added
        return ((new_max, run_sum, mixed), None)

    carried = initial
    piece_rows = gathered_by_axis(key_value, (("ep_0", "ep_1"), "ep_2"), (0, 1), 0)
    piece_count = piece_rows.shape[0]
    length = span_length(piece_count)
    spans = piece_rows.reshape(piece_count // length, length, kv_heads, 2, head_size)
    carried, unused = lax.scan(one_span, carried, spans)
    run_max, run_sum, mixed = carried
    result = (mixed / run_sum[..., None]).astype(jnp.bfloat16)
    result = result.reshape(kv_heads, group, row_count, head_size).transpose(2, 0, 1, 3)
    return result.reshape(row_count, q_heads * head_size)


def ring(step):
    return [(i, (i + step) % 4) for i in range(4)]


def token_slots(own_routes, capacity):
    rows = own_routes.shape[0]
    earlier = jnp.arange(rows)[:, None] < jnp.arange(rows)[None, :]
    slots = []
    for k in range(own_routes.shape[1]):
        mine = own_routes[:, k]
        same = own_routes[:, 0][:, None] == mine[None, :]
        for other in range(1, own_routes.shape[1]):
            same = same | (own_routes[:, other][:, None] == mine[None, :])
        rank = jnp.sum((same & earlier).astype(jnp.int32), axis=0)
        slots.append(mine * capacity + rank)
    return slots


def from_ring(array):
    half = array.shape[0] // 2
    left = lax.ppermute(array, "tp", ring(1))
    right = lax.ppermute(array, "tp", ring(3))
    far = jnp.concatenate(
        [
            lax.ppermute(left[:half], "tp", ring(1)),
            lax.ppermute(right[half:], "tp", ring(3)),
        ]
    )
    return [array, left, right, far]


def hidden_rows(rows_in, w_gate, w_up):
    gate_proj = jnp.dot(rows_in, w_gate, preferred_element_type=jnp.float32)
    up_proj = jnp.dot(rows_in, w_up, preferred_element_type=jnp.float32)
    return (jax.nn.silu(gate_proj) * up_proj).astype(jnp.bfloat16)


def experts_half(
    moe_tokens,
    norm_gain,
    routes,
    route_weights,
    expert_gate,
    expert_up,
    expert_down,
    shared_gate,
    shared_up,
    shared_down,
):
    tok_rows, model_width = moe_tokens.shape
    top_count = routes.shape[1]
    ep_size = lax.axis_size(EP)
    experts = ep_size
    capacity = 2 * tok_rows * top_count // experts
    lane = lax.axis_index("tp")
    values32 = moe_tokens.astype(jnp.float32)
    normed = (
        values32
        * lax.rsqrt(jnp.mean(values32 * values32, axis=-1, keepdims=True) + epsilon)
        * norm_gain
    ).astype(jnp.bfloat16)
    own_routes = lax.dynamic_slice_in_dim(routes, lane * tok_rows, tok_rows, 0)
    own_weights = lax.dynamic_slice_in_dim(route_weights, lane * tok_rows, tok_rows, 0)
    gates = own_weights / jnp.sum(own_weights, axis=-1, keepdims=True) * routed_scale
    slots = token_slots(own_routes, capacity)
    places = jnp.arange(experts * capacity, dtype=jnp.int32)
    one_hots = [(places[:, None] == slot[None, :]).astype(jnp.bfloat16) for slot in slots]
    placed = one_hots[0] + one_hots[1]
    send = jnp.dot(placed, normed, preferred_element_type=jnp.float32).astype(jnp.bfloat16)
    arrived = lax.all_to_all(
        send.reshape(experts, capacity, model_width), EP, split_axis=0, concat_axis=0, tiled=True
    ).reshape(experts * capacity, model_width)
    gate_parts = from_ring(expert_gate[0])
    up_parts = from_ring(expert_up[0])
    down_parts = from_ring(expert_down[0])
    total = None
    for w_gate, w_up, w_down in zip(gate_parts, up_parts, down_parts):
        hidden = hidden_rows(arrived, w_gate, w_up)
        part = jnp.dot(hidden, w_down, preferred_element_type=jnp.float32)
        part = part.astype(jnp.bfloat16).astype(jnp.float32)
        total = part if total is None else total + part
    outgoing = total.astype(jnp.bfloat16).reshape(experts, capacity, model_width)
    returned = lax.all_to_all(outgoing, EP, split_axis=0, concat_axis=0, tiled=True)
    returned = returned.reshape(experts * capacity, model_width)
    group_rows = lax.all_gather(normed, "tp", axis=0, tiled=True)
    shared_hidden = hidden_rows(group_rows, shared_gate, shared_up)
    shared_part = jnp.dot(shared_hidden, shared_down, preferred_element_type=jnp.float32)
    shared_part = shared_part.astype(jnp.bfloat16).reshape(4, tok_rows, model_width)
    shared_got = lax.all_to_all(shared_part, "tp", split_axis=0, concat_axis=0, tiled=True)
    shared_sum = jnp.sum(shared_got.astype(jnp.float32), axis=0)
    routed_total = 0.0
    for k in range(top_count):
        picked = lax.dot_general(
            one_hots[k], returned, (((0,), (0,)), ((), ())), preferred_element_type=jnp.float32
        )
        routed_total = routed_total + gates[:, k : k + 1] * picked
    return (routed_total + shared_sum).astype(jnp.bfloat16)


def body(
    query_rows,
    key_rows,
    value_rows,
    query_gain,
    key_gain,
    moe_tokens,
    norm_gain,
    routes,
    route_weights,
    expert_gate,
    expert_up,
    expert_down,
    shared_gate,
    shared_up,
    shared_down,
):
    attn_out = attend(query_rows, key_rows, value_rows, query_gain, key_gain)
    moe_out = experts_half(
        moe_tokens,
        norm_gain,
        routes,
        route_weights,
        expert_gate,
        expert_up,
        expert_down,
        shared_gate,
        shared_up,
        shared_down,
    )
    return (attn_out, moe_out)


def solution(mesh):
    finer = Mesh(mesh.devices.reshape(8, 4, 2, mesh.shape["tp"]), ("ep_0", "ep_1", "ep_2", "tp"))
    return jax.shard_map(
        body,
        mesh=finer,
        in_specs=(
            P(EP, "tp"),
            P(EP, "tp"),
            P(EP, "tp"),
            P(),
            P(),
            P(EP_TP, None),
            P(),
            P(EP, None),
            P(EP, None),
            P(EP, None, "tp"),
            P(EP, None, "tp"),
            P(EP, "tp", None),
            P(None, "tp"),
            P(None, "tp"),
            P("tp", None),
        ),
        out_specs=(P(EP, "tp"), P(EP_TP, None)),
        check_vma=False,
    )
```

```python
import functools

import jax
import jax.numpy as jnp
from jax import lax
from jax.experimental import pallas as pl
from jax.experimental.pallas import tpu as pltpu
from jax.sharding import Mesh
from jax.sharding import PartitionSpec as P

GRID_W = 64
EP = ("ep_0", "ep_1", "ep_2")
EP_TP = ("ep_0", "ep_1", "ep_2", "tp")
MESH_ID = pl.DeviceIdType.MESH
Z, X, CORE, Y = EP_TP


epsilon = 1e-06
rotary_base = 10000.0
routed_scale = 2.5


def lane_places(heads, size, offset):
    source = jnp.arange(heads * size)[None, :, None]
    lane = jnp.arange(128)[None, None, :] - offset
    head = jnp.arange(heads)[:, None, None]
    inside = (lane >= 0) & (lane < size)
    straight = inside & (source == head * size + lane)
    swapped = inside & (source == head * size + (lane ^ 1))
    return straight.astype(jnp.bfloat16), swapped.astype(jnp.bfloat16)


def rotated(rows_in, gain, heads, size, positions):
    straight, swapped = lane_places(heads, size, 0)
    own = jnp.einsum("td,hde->hte", rows_in, straight, preferred_element_type=jnp.float32)
    other = jnp.einsum("td,hde->hte", rows_in, swapped, preferred_element_type=jnp.float32)
    lane = jnp.arange(128)
    wide = jnp.pad(gain, (0, 128 - size))
    wide_swapped = jnp.pad(gain.reshape(-1, 2)[:, ::-1].reshape(-1), (0, 128 - size))
    factor = lax.rsqrt(jnp.sum(own * own, axis=-1, keepdims=True) / size + epsilon)
    pair_count = size // 4
    pair = (lane // 2) % (2 * pair_count)
    inv_freq = rotary_base ** (-(pair % pair_count).astype(jnp.float32) / pair_count)
    grid_row = (positions // GRID_W).astype(jnp.float32)[:, None]
    grid_col = (positions % GRID_W).astype(jnp.float32)[:, None]
    angles = jnp.where(pair[None, :] < pair_count, grid_row, grid_col) * inv_freq[None, :]
    sign = jnp.where(lane % 2 == 0, -1.0, 1.0)
    turned = (own * factor * wide) * jnp.cos(angles) + (other * factor * wide_swapped) * (
        sign * jnp.sin(angles)
    )
    return turned.astype(jnp.bfloat16)


def attention_kernel(
    q_ref, kv_ref, gate_ref, up_ref,
    out_ref, gates_ref, ups_ref,
    buf, run_max, run_sum, mixed,
    z_send, z_recv, x_send, x_recv, c_send, c_recv, w_send, w_recv, own_sem,
):
    z, x, core, y = (lax.axis_index(name) for name in EP_TP)
    z_size, x_size, y_size = buf.shape[2], buf.shape[1], 4
    half = gate_ref.shape[0] // 2
    block_half = z_size // 2

    def near(index, step, size):
        return lax.rem(index + step + size, size)

    x_right, x_left, x_far = near(x, 1, x_size), near(x, -1, x_size), near(x, 2, x_size)
    y_right, y_left = near(y, 1, y_size), near(y, -1, y_size)
    barrier = pltpu.get_barrier_semaphore()
    peers = [{Z: near(z, k, z_size)} for k in range(1, z_size)]
    peers += [{X: x_right}, {X: x_left}, {CORE: 1 - core}, {Y: y_right}, {Y: y_left}]
    for peer in peers:
        pl.semaphore_signal(barrier, inc=1, device_id=peer, device_id_type=MESH_ID)
    pl.semaphore_wait(barrier, len(peers))

    def remote(src, dst, send_sem, recv_sem, peer):
        return pltpu.make_async_remote_copy(
            src_ref=src, dst_ref=dst, send_sem=send_sem, recv_sem=recv_sem,
            device_id=peer, device_id_type=MESH_ID,
        )

    weights = []
    for n, (source, slots) in enumerate(((gate_ref, gates_ref), (up_ref, ups_ref))):
        to_right = remote(source, slots.at[0], w_send.at[n, 0], w_recv.at[n, 0], {Y: y_right})
        to_left = remote(source, slots.at[1], w_send.at[n, 1], w_recv.at[n, 1], {Y: y_left})
        first, second = pl.ds(0, half), pl.ds(half, half)
        on_right = remote(
            slots.at[0, first], slots.at[2, first], w_send.at[n, 2], w_recv.at[n, 2], {Y: y_right}
        )
        on_left = remote(
            slots.at[1, second], slots.at[2, second], w_send.at[n, 3], w_recv.at[n, 3], {Y: y_left}
        )
        weights.append((to_right, to_left, on_right, on_left))
    for to_right, to_left, _, _ in weights:
        to_right.start()
        to_left.start()

    along_z = [
        remote(kv_ref, buf.at[core, x, z], z_send.at[k], z_recv.at[k], {Z: near(z, k, z_size)})
        for k in range(1, z_size)
    ]
    for copy in along_z:
        copy.start()
    own = pltpu.make_async_copy(kv_ref, buf.at[core, x, z], own_sem)
    own.start()
    run_max[...] = jnp.full_like(run_max, -jnp.inf)
    run_sum[...] = jnp.zeros_like(run_sum)
    mixed[...] = jnp.zeros_like(mixed)
    own.wait()
    for copy in along_z:
        copy.wait_recv()

    def attend(which_core, which_x):
        keys = buf.shape[2] * buf.shape[3]

        def tile(i, carry):
            rows = pl.ds(i * TILE, TILE)
            span = buf[which_core, which_x].reshape(keys, 128)
            scores = lax.dot_general(
                q_ref[rows, :], span, (((1,), (1,)), ((), ())), preferred_element_type=jnp.float32
            )
            old_max = run_max[rows, :]
            new_max = jnp.maximum(old_max, jnp.max(scores, axis=1, keepdims=True))
            factor = jnp.exp(old_max - new_max)
            weights_now = jnp.exp(scores - new_max[:, :1])
            run_sum[rows, :] = run_sum[rows, :] * factor + jnp.sum(
                weights_now, axis=1, keepdims=True
            )
            mixed[rows, :] = mixed[rows, :] * factor + jnp.dot(
                weights_now.astype(jnp.bfloat16), span, preferred_element_type=jnp.float32
            )
            run_max[rows, :] = new_max
            return carry

        lax.fori_loop(0, q_ref.shape[0] // TILE, tile, 0)

    def line_to_core(which_x, slot):
        return remote(
            buf.at[core, which_x], buf.at[core, which_x], c_send.at[slot], c_recv.at[slot],
            {CORE: 1 - core},
        )

    line = buf.at[core, x]
    to_right = remote(line, line, x_send.at[0], x_recv.at[0], {X: x_right})
    to_left = remote(line, line, x_send.at[1], x_recv.at[1], {X: x_left})
    first, second = pl.ds(0, block_half), pl.ds(block_half, block_half)
    on_right = remote(
        buf.at[core, x_left, first], buf.at[core, x_left, first],
        x_send.at[2], x_recv.at[2], {X: x_right},
    )
    on_left = remote(
        buf.at[core, x_right, second], buf.at[core, x_right, second],
        x_send.at[3], x_recv.at[3], {X: x_left},
    )
    lines = [line_to_core(which, n) for n, which in enumerate((x, x_left, x_right, x_far))]
    to_right.start()
    to_left.start()
    lines[0].start()
    attend(core, x)
    lines[0].wait_recv()
    attend(1 - core, x)
    to_right.wait_recv()
    on_right.start()
    lines[1].start()
    to_left.wait_recv()
    on_left.start()
    lines[2].start()
    attend(core, x_left)
    weights[0][0].wait_recv()
    weights[0][2].start()
    weights[0][1].wait_recv()
    weights[0][3].start()
    attend(core, x_right)
    on_right.wait_recv()
    on_left.wait_recv()
    lines[3].start()
    lines[1].wait_recv()
    attend(1 - core, x_left)
    weights[1][0].wait_recv()
    weights[1][2].start()
    weights[1][1].wait_recv()
    weights[1][3].start()
    lines[2].wait_recv()
    attend(1 - core, x_right)
    attend(core, x_far)
    lines[3].wait_recv()
    attend(1 - core, x_far)
    out_ref[...] = (mixed[...] / run_sum[...]).astype(out_ref.dtype)
    for group in weights:
        group[2].wait_recv()
        group[3].wait_recv()
        for copy in group:
            copy.wait_send()
    for copy in along_z + [to_right, to_left, on_right, on_left] + lines:
        copy.wait_send()


TILE = 256


def attend_and_gather(q_rows, key_value, w_gate, w_up):
    rows = q_rows.shape[0]
    tokens = key_value.shape[0]
    z_size, x_size, cores = (lax.axis_size(name) for name in EP)
    dma = pltpu.SemaphoreType.DMA
    slots = jax.ShapeDtypeStruct((3, *w_gate.shape), w_gate.dtype)
    vmem, anywhere = pl.BlockSpec(memory_space=pltpu.VMEM), pl.BlockSpec(memory_space=pl.ANY)
    keys = tokens * z_size * x_size * cores
    return pl.pallas_call(
        attention_kernel,
        out_shape=[jax.ShapeDtypeStruct((rows, 128), jnp.bfloat16), slots, slots],
        in_specs=[vmem, vmem, anywhere, anywhere],
        out_specs=[vmem, anywhere, anywhere],
        scratch_shapes=[
            pltpu.VMEM((cores, x_size, z_size, tokens, 128), jnp.bfloat16),
            pltpu.VMEM((rows, 128), jnp.float32),
            pltpu.VMEM((rows, 128), jnp.float32),
            pltpu.VMEM((rows, 128), jnp.float32),
            dma((z_size,)), dma((z_size,)),
            dma((4,)), dma((4,)),
            dma((4,)), dma((4,)),
            dma((2, 4)), dma((2, 4)),
            dma,
        ],
        compiler_params=pltpu.CompilerParams(
            collective_id=0, has_side_effects=True, vmem_limit_bytes=40 * 1024 * 1024
        ),
        cost_estimate=pl.CostEstimate(
            flops=60 * rows * keys * 128 // 2, bytes_accessed=2 * keys * 256, transcendentals=0
        ),
        name="attend_and_gather",
    )(q_rows, key_value, w_gate, w_up)


def ring(step):
    return [(i, (i + step) % 4) for i in range(4)]


def token_slots(own_routes, capacity):
    rows = own_routes.shape[0]
    earlier = jnp.arange(rows)[:, None] < jnp.arange(rows)[None, :]
    slots = []
    for k in range(own_routes.shape[1]):
        mine = own_routes[:, k]
        same = own_routes[:, 0][:, None] == mine[None, :]
        for other in range(1, own_routes.shape[1]):
            same = same | (own_routes[:, other][:, None] == mine[None, :])
        rank = jnp.sum((same & earlier).astype(jnp.int32), axis=0)
        slots.append(mine * capacity + rank)
    return slots


def from_ring(array):
    half = array.shape[0] // 2
    left = lax.ppermute(array, "tp", ring(1))
    right = lax.ppermute(array, "tp", ring(3))
    far = jnp.concatenate(
        [
            lax.ppermute(left[:half], "tp", ring(1)),
            lax.ppermute(right[half:], "tp", ring(3)),
        ]
    )
    return [array, left, right, far]


def hidden_rows(rows_in, w_gate, w_up):
    gate_proj = jnp.dot(rows_in, w_gate, preferred_element_type=jnp.float32)
    up_proj = jnp.dot(rows_in, w_up, preferred_element_type=jnp.float32)
    return (jax.nn.silu(gate_proj) * up_proj).astype(jnp.bfloat16)


def dispatch(
    moe_tokens,
    norm_gain,
    routes,
    route_weights,
):
    tok_rows, model_width = moe_tokens.shape
    top_count = routes.shape[1]
    ep_size = lax.axis_size(EP)
    experts = ep_size
    capacity = 2 * tok_rows * top_count // experts
    lane = lax.axis_index("tp")
    values32 = moe_tokens.astype(jnp.float32)
    normed = (
        values32
        * lax.rsqrt(jnp.mean(values32 * values32, axis=-1, keepdims=True) + epsilon)
        * norm_gain
    ).astype(jnp.bfloat16)
    own_routes = lax.dynamic_slice_in_dim(routes, lane * tok_rows, tok_rows, 0)
    own_weights = lax.dynamic_slice_in_dim(route_weights, lane * tok_rows, tok_rows, 0)
    gates = own_weights / jnp.sum(own_weights, axis=-1, keepdims=True) * routed_scale
    slots = token_slots(own_routes, capacity)
    places = jnp.arange(experts * capacity, dtype=jnp.int32)
    one_hots = [(places[:, None] == slot[None, :]).astype(jnp.bfloat16) for slot in slots]
    placed = one_hots[0] + one_hots[1]
    send = jnp.dot(placed, normed, preferred_element_type=jnp.float32).astype(jnp.bfloat16)
    arrived = lax.all_to_all(
        send.reshape(experts, capacity, model_width), EP, split_axis=0, concat_axis=0, tiled=True
    ).reshape(experts * capacity, model_width)
    return normed, arrived, one_hots, gates


def experts_half(
    dispatched,
    gates_got,
    ups_got,
    expert_gate,
    expert_up,
    expert_down,
    shared_gate,
    shared_up,
    shared_down,
):
    normed, arrived, one_hots, gates = dispatched
    tok_rows, model_width = normed.shape
    experts = lax.axis_size(EP)
    capacity = arrived.shape[0] // experts
    top_count = len(one_hots)
    gate_parts = [expert_gate[0], gates_got[0], gates_got[1], gates_got[2]]
    up_parts = [expert_up[0], ups_got[0], ups_got[1], ups_got[2]]
    down_parts = from_ring(expert_down[0])
    total = None
    for w_gate, w_up, w_down in zip(gate_parts, up_parts, down_parts):
        hidden = hidden_rows(arrived, w_gate, w_up)
        part = jnp.dot(hidden, w_down, preferred_element_type=jnp.float32)
        part = part.astype(jnp.bfloat16).astype(jnp.float32)
        total = part if total is None else total + part
    outgoing = total.astype(jnp.bfloat16).reshape(experts, capacity, model_width)
    returned = lax.all_to_all(outgoing, EP, split_axis=0, concat_axis=0, tiled=True)
    returned = returned.reshape(experts * capacity, model_width)
    group_rows = lax.all_gather(normed, "tp", axis=0, tiled=True)
    shared_hidden = hidden_rows(group_rows, shared_gate, shared_up)
    shared_part = jnp.dot(shared_hidden, shared_down, preferred_element_type=jnp.float32)
    shared_part = shared_part.astype(jnp.bfloat16).reshape(4, tok_rows, model_width)
    shared_got = lax.all_to_all(shared_part, "tp", split_axis=0, concat_axis=0, tiled=True)
    shared_sum = jnp.sum(shared_got.astype(jnp.float32), axis=0)
    routed_total = 0.0
    for k in range(top_count):
        picked = lax.dot_general(
            one_hots[k], returned, (((0,), (0,)), ((), ())), preferred_element_type=jnp.float32
        )
        routed_total = routed_total + gates[:, k : k + 1] * picked
    return (routed_total + shared_sum).astype(jnp.bfloat16)


def body(
    query_rows,
    key_rows,
    value_rows,
    query_gain,
    key_gain,
    moe_tokens,
    norm_gain,
    routes,
    route_weights,
    expert_gate,
    expert_up,
    expert_down,
    shared_gate,
    shared_up,
    shared_down,
):
    dispatched = dispatch(moe_tokens, norm_gain, routes, route_weights)
    row_count = query_rows.shape[0]
    size = query_gain.shape[0]
    heads = query_rows.shape[1] // size
    positions = lax.axis_index(EP) * row_count + jnp.arange(row_count, dtype=jnp.int32)
    q_rot = rotated(query_rows, query_gain, heads, size, positions) * jnp.bfloat16(size**-0.5)
    k_rot = rotated(key_rows, key_gain, 1, size, positions)[0]
    placed = lane_places(1, size, size)[0][0]
    values = jnp.dot(value_rows, placed, preferred_element_type=jnp.float32).astype(jnp.bfloat16)
    attn, gates_got, ups_got = attend_and_gather(
        q_rot.reshape(heads * row_count, 128), k_rot + values, expert_gate[0], expert_up[0]
    )
    attn_out = attn[:, size:].reshape(heads, row_count, size).transpose(1, 0, 2)
    attn_out = attn_out.reshape(row_count, heads * size)
    moe_out = experts_half(
        dispatched,
        gates_got,
        ups_got,
        expert_gate,
        expert_up,
        expert_down,
        shared_gate,
        shared_up,
        shared_down,
    )
    return (attn_out, moe_out)


def solution(mesh):
    finer = Mesh(mesh.devices.reshape(8, 4, 2, mesh.shape["tp"]), ("ep_0", "ep_1", "ep_2", "tp"))
    return jax.shard_map(
        body,
        mesh=finer,
        in_specs=(
            P(EP, "tp"),
            P(EP, "tp"),
            P(EP, "tp"),
            P(),
            P(),
            P(EP_TP, None),
            P(),
            P(EP, None),
            P(EP, None),
            P(EP, None, "tp"),
            P(EP, None, "tp"),
            P(EP, "tp", None),
            P(None, "tp"),
            P(None, "tp"),
            P("tp", None),
        ),
        out_specs=(P(EP, "tp"), P(EP_TP, None)),
        check_vma=False,
    )
```

```python
import functools

import jax
import jax.numpy as jnp
from jax import lax
from jax.experimental import pallas as pl
from jax.experimental.pallas import tpu as pltpu
from jax.sharding import Mesh
from jax.sharding import PartitionSpec as P

GRID_W = 64
EP = ("ep_0", "ep_1", "ep_2")
EP_TP = ("ep_0", "ep_1", "ep_2", "tp")
MESH_ID = pl.DeviceIdType.MESH
Z, X, CORE, Y = EP_TP


epsilon = 1e-06
rotary_base = 10000.0
routed_scale = 2.5


def lane_places(heads, size, offset):
    source = jnp.arange(heads * size)[None, :, None]
    lane = jnp.arange(128)[None, None, :] - offset
    head = jnp.arange(heads)[:, None, None]
    inside = (lane >= 0) & (lane < size)
    straight = inside & (source == head * size + lane)
    swapped = inside & (source == head * size + (lane ^ 1))
    return straight.astype(jnp.bfloat16), swapped.astype(jnp.bfloat16)


def rotated(rows_in, gain, heads, size, positions):
    straight, swapped = lane_places(heads, size, 0)
    own = jnp.einsum("td,hde->hte", rows_in, straight, preferred_element_type=jnp.float32)
    other = jnp.einsum("td,hde->hte", rows_in, swapped, preferred_element_type=jnp.float32)
    lane = jnp.arange(128)
    wide = jnp.pad(gain, (0, 128 - size))
    wide_swapped = jnp.pad(gain.reshape(-1, 2)[:, ::-1].reshape(-1), (0, 128 - size))
    factor = lax.rsqrt(jnp.sum(own * own, axis=-1, keepdims=True) / size + epsilon)
    pair_count = size // 4
    pair = (lane // 2) % (2 * pair_count)
    inv_freq = rotary_base ** (-(pair % pair_count).astype(jnp.float32) / pair_count)
    grid_row = (positions // GRID_W).astype(jnp.float32)[:, None]
    grid_col = (positions % GRID_W).astype(jnp.float32)[:, None]
    angles = jnp.where(pair[None, :] < pair_count, grid_row, grid_col) * inv_freq[None, :]
    sign = jnp.where(lane % 2 == 0, -1.0, 1.0)
    turned = (own * factor * wide) * jnp.cos(angles) + (other * factor * wide_swapped) * (
        sign * jnp.sin(angles)
    )
    return turned.astype(jnp.bfloat16)


def token_slots(own_routes, capacity):
    rows = own_routes.shape[0]
    earlier = jnp.arange(rows)[:, None] < jnp.arange(rows)[None, :]
    slots = []
    for k in range(own_routes.shape[1]):
        mine = own_routes[:, k]
        same = own_routes[:, 0][:, None] == mine[None, :]
        for other in range(1, own_routes.shape[1]):
            same = same | (own_routes[:, other][:, None] == mine[None, :])
        rank = jnp.sum((same & earlier).astype(jnp.int32), axis=0)
        slots.append(mine * capacity + rank)
    return slots


CHUNKS = 4
TILE = 256


def layer_kernel(
    q_ref, kv_ref, send_ref, normed_ref, pick_ref, scale_ref,
    gate_ref, up_ref, down_ref, shared_gate_ref, shared_up_ref, shared_down_ref,
    attn_ref, moe_ref,
    buf, run_max, run_sum, mixed,
    w_gate, w_up, w_down, s_gate, s_up, s_down,
    arrived, rows, hidden, out, returned,
    group, part, part_in, relay,
    z_send, z_recv, x_send, x_recv, c_send, c_recv, w_send, w_recv, d_send, d_recv,
    disp_send, disp_recv, ret_send, ret_recv, g_send, g_recv, p_send, p_recv, own_sem,
):
    z, x, core, y = (lax.axis_index(name) for name in EP_TP)
    z_size, x_size, cores, y_size = buf.shape[2], buf.shape[1], buf.shape[0], 4
    experts, capacity = arrived.shape[0], arrived.shape[1]
    model_width = normed_ref.shape[1]
    tokens = normed_ref.shape[0]
    width = model_width // CHUNKS
    me = (z * x_size + x) * cores + core

    def near(index, step, size):
        return lax.rem(index + step + size, size)

    def member(index):
        return {
            Z: index // (x_size * cores),
            X: lax.rem(index // cores, x_size),
            CORE: lax.rem(index, cores),
        }

    def remote(src, dst, send_sem, recv_sem, peer):
        return pltpu.make_async_remote_copy(
            src_ref=src, dst_ref=dst, send_sem=send_sem, recv_sem=recv_sem,
            device_id=peer, device_id_type=MESH_ID,
        )

    x_right, x_left, x_far = near(x, 1, x_size), near(x, -1, x_size), near(x, 2, x_size)
    right, left = {Y: near(y, 1, y_size)}, {Y: near(y, -1, y_size)}
    barrier = pltpu.get_barrier_semaphore()

    def greet(k, carry):
        pl.semaphore_signal(
            barrier, inc=1, device_id=member(lax.rem(me + k, experts)), device_id_type=MESH_ID
        )
        return carry

    lax.fori_loop(1, experts, greet, 0)
    for peer in (right, left):
        pl.semaphore_signal(barrier, inc=1, device_id=peer, device_id_type=MESH_ID)
    pl.semaphore_wait(barrier, experts + 1)

    def ring_copies(slots, own_source, pick, size, send_sems, recv_sems):
        first, second = pl.ds(0, size // 2), pl.ds(size // 2, size // 2)
        return (
            remote(own_source, pick(slots, 1), send_sems.at[0], recv_sems.at[0], right),
            remote(own_source, pick(slots, 2), send_sems.at[1], recv_sems.at[1], left),
            remote(
                pick(slots, 1, first), pick(slots, 3, first), send_sems.at[2], recv_sems.at[2], right
            ),
            remote(
                pick(slots, 2, second), pick(slots, 3, second), send_sems.at[3], recv_sems.at[3], left
            ),
        )

    def whole(slots, slot, span=None):
        return slots.at[slot] if span is None else slots.at[slot, span]

    depth = gate_ref.shape[0]
    gates = ring_copies(w_gate, gate_ref, whole, depth, w_send.at[0], w_recv.at[0])
    ups = ring_copies(w_up, up_ref, whole, depth, w_send.at[1], w_recv.at[1])
    downs = []
    units = down_ref.shape[0]
    for n in range(CHUNKS):
        columns = pl.ds(n * width, width)

        def some(slots, slot, span=None, columns=columns):
            return slots.at[slot, pl.ds(0, units) if span is None else span, columns]

        downs.append(
            ring_copies(
                w_down, down_ref.at[:, columns], some, units, d_send.at[n], d_recv.at[n]
            )
        )

    def start_both(ring):
        ring[0].start()
        ring[1].start()

    def pass_on(ring):
        ring[0].wait_recv()
        ring[2].start()
        ring[1].wait_recv()
        ring[3].start()

    def far_arrived(ring):
        ring[2].wait_recv()
        ring[3].wait_recv()

    start_both(gates)
    start_both(ups)

    along_z = [
        remote(kv_ref, buf.at[core, x, z], z_send.at[k], z_recv.at[k], {Z: near(z, k, z_size)})
        for k in range(1, z_size)
    ]
    for copy in along_z:
        copy.start()

    def send_rows(i, carry):
        to = lax.rem(me + lax.rem(i * 13, experts), experts)
        remote(send_ref.at[to], arrived.at[me], disp_send, disp_recv, member(to)).start()
        return carry

    lax.fori_loop(1, experts, send_rows, 0)
    locals_ = [
        pltpu.make_async_copy(source, target, own_sem.at[n])
        for n, (source, target) in enumerate((
            (kv_ref, buf.at[core, x, z]),
            (send_ref.at[me], arrived.at[me]),
            (gate_ref, w_gate.at[0]),
            (up_ref, w_up.at[0]),
            (down_ref, w_down.at[0]),
            (shared_gate_ref, s_gate),
            (shared_up_ref, s_up),
            (shared_down_ref, s_down),
            (normed_ref, group.at[0]),
        ))
    ]
    for copy in locals_:
        copy.start()
    run_max[...] = jnp.full_like(run_max, -jnp.inf)
    run_sum[...] = jnp.zeros_like(run_sum)
    mixed[...] = jnp.zeros_like(mixed)
    locals_[0].wait()
    for copy in along_z:
        copy.wait_recv()

    def attend(which_core, which_x):
        keys = buf.shape[2] * buf.shape[3]

        def tile(i, carry):
            here = pl.ds(i * TILE, TILE)
            span = buf[which_core, which_x].reshape(keys, 128)
            scores = lax.dot_general(
                q_ref[here, :], span, (((1,), (1,)), ((), ())), preferred_element_type=jnp.float32
            )
            old_max = run_max[here, :]
            new_max = jnp.maximum(old_max, jnp.max(scores, axis=1, keepdims=True))
            factor = jnp.exp(old_max - new_max)
            weights_now = jnp.exp(scores - new_max[:, :1])
            run_sum[here, :] = run_sum[here, :] * factor + jnp.sum(
                weights_now, axis=1, keepdims=True
            )
            mixed[here, :] = mixed[here, :] * factor + jnp.dot(
                weights_now.astype(jnp.bfloat16), span, preferred_element_type=jnp.float32
            )
            run_max[here, :] = new_max
            return carry

        lax.fori_loop(0, q_ref.shape[0] // TILE, tile, 0)

    def line_to_core(which_x, slot):
        return remote(
            buf.at[core, which_x], buf.at[core, which_x], c_send.at[slot], c_recv.at[slot],
            {CORE: 1 - core},
        )

    line = buf.at[core, x]
    to_right = remote(line, line, x_send.at[0], x_recv.at[0], {X: x_right})
    to_left = remote(line, line, x_send.at[1], x_recv.at[1], {X: x_left})
    first, second = pl.ds(0, z_size // 2), pl.ds(z_size // 2, z_size // 2)
    on_right = remote(
        buf.at[core, x_left, first], buf.at[core, x_left, first],
        x_send.at[2], x_recv.at[2], {X: x_right},
    )
    on_left = remote(
        buf.at[core, x_right, second], buf.at[core, x_right, second],
        x_send.at[3], x_recv.at[3], {X: x_left},
    )
    lines = [line_to_core(which, n) for n, which in enumerate((x, x_left, x_right, x_far))]
    to_right.start()
    to_left.start()
    lines[0].start()
    attend(core, x)
    lines[0].wait_recv()
    attend(1 - core, x)
    to_right.wait_recv()
    on_right.start()
    lines[1].start()
    to_left.wait_recv()
    on_left.start()
    lines[2].start()
    pass_on(gates)
    attend(core, x_left)
    attend(core, x_right)
    on_right.wait_recv()
    on_left.wait_recv()
    lines[3].start()
    lines[1].wait_recv()
    pass_on(ups)
    for n in range(CHUNKS):
        start_both(downs[n])
    attend(1 - core, x_left)
    lines[2].wait_recv()
    attend(1 - core, x_right)
    attend(core, x_far)
    lines[3].wait_recv()
    attend(1 - core, x_far)
    attn_ref[...] = (mixed[...] / run_sum[...]).astype(attn_ref.dtype)

    others = pl.ds(0, experts - 1)
    pltpu.make_async_copy(arrived.at[others], arrived.at[others], disp_recv).wait()
    for copy in locals_[1:]:
        copy.wait()

    def flatten(i, carry):
        block = arrived[pl.ds(i * 8, 8)].astype(jnp.float32).reshape(8 * capacity, model_width)
        rows[pl.ds(i * 8 * capacity, 8 * capacity), :] = block.astype(jnp.bfloat16)
        return carry

    lax.fori_loop(0, experts // 8, flatten, 0)

    def activated(source, gate_now, up_now):
        gate_proj = jnp.dot(source, gate_now, preferred_element_type=jnp.float32)
        up_proj = jnp.dot(source, up_now, preferred_element_type=jnp.float32)
        return (gate_proj / (1.0 + jnp.exp(-gate_proj)) * up_proj).astype(jnp.bfloat16)

    def fill_hidden(slot):
        def tile(i, carry):
            here = pl.ds(i * TILE, TILE)
            hidden[here, slot * units : (slot + 1) * units] = activated(
                rows[here, :], w_gate[slot], w_up[slot]
            )
            return carry

        lax.fori_loop(0, rows.shape[0] // TILE, tile, 0)

    for slot in range(3):
        fill_hidden(slot)
    pass_on(downs[0])
    far_arrived(gates)
    far_arrived(ups)
    fill_hidden(3)
    shared_ring = ring_copies(group, normed_ref, whole, tokens, g_send, g_recv)
    for n in range(CHUNKS):
        if n + 1 < CHUNKS:
            pass_on(downs[n + 1])
        else:
            start_both(shared_ring)
        far_arrived(downs[n])

        def product(i, carry, n=n):
            here = pl.ds(i * TILE, TILE)
            value = jnp.dot(
                hidden[here, :],
                w_down[:, :, n * width : (n + 1) * width].reshape(4 * units, width),
                preferred_element_type=jnp.float32,
            )
            count = TILE // capacity
            out[n, pl.ds(i * count, count)] = value.reshape(count, capacity, width).astype(
                jnp.bfloat16
            )
            return carry

        lax.fori_loop(0, rows.shape[0] // TILE, product, 0)

        def send_back(i, carry, n=n):
            to = lax.rem(me + lax.rem(i * 13, experts), experts)
            remote(
                out.at[n, to], returned.at[n, me], ret_send.at[n], ret_recv.at[n], member(to)
            ).start()
            return carry

        lax.fori_loop(1, experts, send_back, 0)
        pltpu.make_async_copy(out.at[n, me], returned.at[n, me], own_sem.at[9 + n]).start()

    pass_on(shared_ring)

    def shared_part(slot):
        value = activated(group[slot], s_gate[...], s_up[...])
        for n in range(CHUNKS):
            columns = slice(n * width, (n + 1) * width)
            part[slot, :, columns] = jnp.dot(
                value, s_down[:, columns], preferred_element_type=jnp.float32
            ).astype(jnp.bfloat16)

    top, bottom = pl.ds(0, tokens // 2), pl.ds(tokens // 2, tokens // 2)
    part_left = remote(part.at[1], part_in.at[2], p_send.at[0], p_recv.at[0], left)
    part_right = remote(part.at[2], part_in.at[1], p_send.at[1], p_recv.at[1], right)
    via_right = remote(part.at[3, top], relay.at[0], p_send.at[2], p_recv.at[2], right)
    via_left = remote(part.at[3, bottom], relay.at[1], p_send.at[3], p_recv.at[3], left)
    on_to_right = remote(relay.at[0], part_in.at[0, top], p_send.at[4], p_recv.at[4], right)
    on_to_left = remote(relay.at[1], part_in.at[0, bottom], p_send.at[5], p_recv.at[5], left)
    shared_part(1)
    part_left.start()
    shared_part(2)
    part_right.start()
    far_arrived(shared_ring)
    shared_part(3)
    via_right.start()
    via_left.start()
    shared_part(0)
    via_right.wait_recv()
    on_to_right.start()
    via_left.wait_recv()
    on_to_left.start()
    part_left.wait_recv()
    part_right.wait_recv()
    on_to_right.wait_recv()
    on_to_left.wait_recv()

    for n in range(CHUNKS):
        pltpu.make_async_copy(
            returned.at[n, others], returned.at[n, others], ret_recv.at[n]
        ).wait()
        pltpu.make_async_copy(out.at[n, me], returned.at[n, me], own_sem.at[9 + n]).wait()
        columns = slice(n * width, (n + 1) * width)
        results = returned[n].astype(jnp.float32).reshape(experts * capacity, width)
        results = results.astype(jnp.bfloat16)
        total = part[0, :, columns].astype(jnp.float32)
        for slot in range(3):
            total = total + part_in[slot, :, columns].astype(jnp.float32)
        routed = None
        for k in range(pick_ref.shape[0]):
            picked = jnp.dot(pick_ref[k], results, preferred_element_type=jnp.float32)
            term = scale_ref[k][:, :1] * picked
            routed = term if routed is None else routed + term
        moe_ref[:, columns] = (routed + total).astype(moe_ref.dtype)

    for ring in [gates, ups, shared_ring] + downs:
        for copy in ring:
            copy.wait_send()
    for copy in along_z + [to_right, to_left, on_right, on_left] + lines:
        copy.wait_send()
    for copy in (part_left, part_right, via_right, via_left, on_to_right, on_to_left):
        copy.wait_send()
    pltpu.make_async_copy(send_ref.at[others], arrived.at[others], disp_send).wait()
    for n in range(CHUNKS):
        pltpu.make_async_copy(out.at[n, others], returned.at[n, others], ret_send.at[n]).wait()


def run_layer(q_rows, key_value, send, normed, picks, scales, expert_weights, shared_weights):
    query_count = q_rows.shape[0]
    tokens = key_value.shape[0]
    z_size, x_size, cores = (lax.axis_size(name) for name in EP)
    experts, capacity, model_width = send.shape
    depth, units = expert_weights[0].shape
    rows, own = experts * capacity, normed.shape[0]
    dma = pltpu.SemaphoreType.DMA
    bf16, f32 = jnp.bfloat16, jnp.float32
    width = model_width // CHUNKS
    vmem, anywhere = pl.BlockSpec(memory_space=pltpu.VMEM), pl.BlockSpec(memory_space=pl.ANY)
    keys = tokens * z_size * x_size * cores
    return pl.pallas_call(
        layer_kernel,
        out_shape=[
            jax.ShapeDtypeStruct((query_count, 128), bf16),
            jax.ShapeDtypeStruct(normed.shape, bf16),
        ],
        in_specs=[vmem, vmem, anywhere, vmem, vmem, vmem] + [anywhere] * 6,
        out_specs=[vmem, vmem],
        scratch_shapes=[
            pltpu.VMEM((cores, x_size, z_size, tokens, 128), bf16),
            pltpu.VMEM((query_count, 128), f32),
            pltpu.VMEM((query_count, 128), f32),
            pltpu.VMEM((query_count, 128), f32),
            pltpu.VMEM((4, depth, units), bf16),
            pltpu.VMEM((4, depth, units), bf16),
            pltpu.VMEM((4, units, depth), bf16),
            pltpu.VMEM((depth, units), bf16),
            pltpu.VMEM((depth, units), bf16),
            pltpu.VMEM((units, depth), bf16),
            pltpu.VMEM((experts, capacity, model_width), bf16),
            pltpu.VMEM((rows, model_width), bf16),
            pltpu.VMEM((rows, 4 * units), bf16),
            pltpu.VMEM((CHUNKS, experts, capacity, width), bf16),
            pltpu.VMEM((CHUNKS, experts, capacity, width), bf16),
            pltpu.VMEM((4, own, model_width), bf16),
            pltpu.VMEM((4, own, model_width), bf16),
            pltpu.VMEM((3, own, model_width), bf16),
            pltpu.VMEM((2, own // 2, model_width), bf16),
            dma((z_size,)), dma((z_size,)),
            dma((4,)), dma((4,)),
            dma((4,)), dma((4,)),
            dma((2, 4)), dma((2, 4)),
            dma((CHUNKS, 4)), dma((CHUNKS, 4)),
            dma, dma,
            dma((CHUNKS,)), dma((CHUNKS,)),
            dma((4,)), dma((4,)),
            dma((6,)), dma((6,)),
            dma((9 + CHUNKS,)),
        ],
        compiler_params=pltpu.CompilerParams(
            collective_id=0, has_side_effects=True, vmem_limit_bytes=60 * 1024 * 1024
        ),
        cost_estimate=pl.CostEstimate(
            flops=60 * query_count * keys * 128 // 2, bytes_accessed=2 * keys * 256, transcendentals=0
        ),
        name="layer",
    )(q_rows, key_value, send, normed, picks, scales, *expert_weights, *shared_weights)


def dispatch(moe_tokens, norm_gain, routes, route_weights):
    tok_rows, model_width = moe_tokens.shape
    top_count = routes.shape[1]
    experts = lax.axis_size(EP)
    capacity = 2 * tok_rows * top_count // experts
    lane = lax.axis_index("tp")
    values32 = moe_tokens.astype(jnp.float32)
    normed = (
        values32
        * lax.rsqrt(jnp.mean(values32 * values32, axis=-1, keepdims=True) + epsilon)
        * norm_gain
    ).astype(jnp.bfloat16)
    own_routes = lax.dynamic_slice_in_dim(routes, lane * tok_rows, tok_rows, 0)
    own_weights = lax.dynamic_slice_in_dim(route_weights, lane * tok_rows, tok_rows, 0)
    gates = own_weights / jnp.sum(own_weights, axis=-1, keepdims=True) * routed_scale
    slots = token_slots(own_routes, capacity)
    places = jnp.arange(experts * capacity, dtype=jnp.int32)
    placed = (places[:, None] == slots[0][None, :]) | (places[:, None] == slots[1][None, :])
    send = jnp.dot(placed.astype(jnp.bfloat16), normed, preferred_element_type=jnp.float32)
    send = send.astype(jnp.bfloat16).reshape(experts, capacity, model_width)
    picks = jnp.stack([(slot[:, None] == places[None, :]).astype(jnp.bfloat16) for slot in slots])
    scales = jnp.broadcast_to(gates.T[:, :, None], (top_count, tok_rows, 128))
    return send, normed, picks, scales


def body(
    query_rows,
    key_rows,
    value_rows,
    query_gain,
    key_gain,
    moe_tokens,
    norm_gain,
    routes,
    route_weights,
    expert_gate,
    expert_up,
    expert_down,
    shared_gate,
    shared_up,
    shared_down,
):
    dispatched = dispatch(moe_tokens, norm_gain, routes, route_weights)
    row_count = query_rows.shape[0]
    size = query_gain.shape[0]
    heads = query_rows.shape[1] // size
    positions = lax.axis_index(EP) * row_count + jnp.arange(row_count, dtype=jnp.int32)
    q_rot = rotated(query_rows, query_gain, heads, size, positions) * jnp.bfloat16(size**-0.5)
    k_rot = rotated(key_rows, key_gain, 1, size, positions)[0]
    placed = lane_places(1, size, size)[0][0]
    values = jnp.dot(value_rows, placed, preferred_element_type=jnp.float32).astype(jnp.bfloat16)
    attn, moe_out = run_layer(
        q_rot.reshape(heads * row_count, 128),
        k_rot + values,
        *dispatched,
        (expert_gate[0], expert_up[0], expert_down[0]),
        (shared_gate, shared_up, shared_down),
    )
    attn_out = attn[:, size:].reshape(heads, row_count, size).transpose(1, 0, 2)
    return (attn_out.reshape(row_count, heads * size), moe_out)


def solution(mesh):
    finer = Mesh(mesh.devices.reshape(8, 4, 2, mesh.shape["tp"]), ("ep_0", "ep_1", "ep_2", "tp"))
    return jax.shard_map(
        body,
        mesh=finer,
        in_specs=(
            P(EP, "tp"),
            P(EP, "tp"),
            P(EP, "tp"),
            P(),
            P(),
            P(EP_TP, None),
            P(),
            P(EP, None),
            P(EP, None),
            P(EP, None, "tp"),
            P(EP, None, "tp"),
            P(EP, "tp", None),
            P(None, "tp"),
            P(None, "tp"),
            P("tp", None),
        ),
        out_specs=(P(EP, "tp"), P(EP_TP, None)),
        check_vma=False,
    )
```

```python
import functools

import jax
import jax.numpy as jnp
from jax import lax
from jax.experimental import pallas as pl
from jax.experimental.pallas import tpu as pltpu
from jax.sharding import Mesh
from jax.sharding import PartitionSpec as P

GRID_W = 64
EP = ("ep_0", "ep_1", "ep_2")
EP_TP = ("ep_0", "ep_1", "ep_2", "tp")
MESH_ID = pl.DeviceIdType.MESH
Z, X, CORE, Y = EP_TP


epsilon = 1e-06
rotary_base = 10000.0
routed_scale = 2.5


def lane_places(heads, size, offset):
    source = jnp.arange(heads * size)[None, :, None]
    lane = jnp.arange(128)[None, None, :] - offset
    head = jnp.arange(heads)[:, None, None]
    inside = (lane >= 0) & (lane < size)
    straight = inside & (source == head * size + lane)
    swapped = inside & (source == head * size + (lane ^ 1))
    return straight.astype(jnp.bfloat16), swapped.astype(jnp.bfloat16)


def rotated(rows_in, gain, heads, size, positions):
    straight, swapped = lane_places(heads, size, 0)
    own = jnp.einsum("td,hde->hte", rows_in, straight, preferred_element_type=jnp.float32)
    other = jnp.einsum("td,hde->hte", rows_in, swapped, preferred_element_type=jnp.float32)
    lane = jnp.arange(128)
    wide = jnp.pad(gain, (0, 128 - size))
    wide_swapped = jnp.pad(gain.reshape(-1, 2)[:, ::-1].reshape(-1), (0, 128 - size))
    factor = lax.rsqrt(jnp.sum(own * own, axis=-1, keepdims=True) / size + epsilon)
    pair_count = size // 4
    pair = (lane // 2) % (2 * pair_count)
    inv_freq = rotary_base ** (-(pair % pair_count).astype(jnp.float32) / pair_count)
    grid_row = (positions // GRID_W).astype(jnp.float32)[:, None]
    grid_col = (positions % GRID_W).astype(jnp.float32)[:, None]
    angles = jnp.where(pair[None, :] < pair_count, grid_row, grid_col) * inv_freq[None, :]
    sign = jnp.where(lane % 2 == 0, -1.0, 1.0)
    turned = (own * factor * wide) * jnp.cos(angles) + (other * factor * wide_swapped) * (
        sign * jnp.sin(angles)
    )
    return turned.astype(jnp.bfloat16)


def ring(step):
    return [(i, (i + step) % 4) for i in range(4)]


def token_slots(own_routes, capacity):
    rows = own_routes.shape[0]
    earlier = jnp.arange(rows)[:, None] < jnp.arange(rows)[None, :]
    slots = []
    for k in range(own_routes.shape[1]):
        mine = own_routes[:, k]
        same = own_routes[:, 0][:, None] == mine[None, :]
        for other in range(1, own_routes.shape[1]):
            same = same | (own_routes[:, other][:, None] == mine[None, :])
        rank = jnp.sum((same & earlier).astype(jnp.int32), axis=0)
        slots.append(mine * capacity + rank)
    return slots


CHUNKS = 4
TILE = 256


def layer_kernel(
    q_ref, kv_ref, send_ref, normed_ref, pick_ref, scale_ref,
    gate_left_ref, gate_right_ref,
    gate_ref, up_ref, down_ref, shared_gate_ref, shared_up_ref, shared_down_ref,
    attn_ref, moe_ref,
    buf, run_max, run_sum, mixed,
    w_gate, w_up, w_down, s_gate, s_up, s_down,
    arrived, rows, hidden, out, returned,
    shared_sum, row_relay, result_relay,
    z_send, z_recv, x_send, x_recv, c_send, c_recv, w_send, w_recv, d_send, d_recv,
    disp_send, disp_recv, ret_send, ret_recv, sy_send, sy_recv, sx_send, sx_recv, sc_send, sc_recv,
    relay_send, relay_recv, own_sem,
):
    z, x, core, y = (lax.axis_index(name) for name in EP_TP)
    z_size, x_size, cores, y_size = buf.shape[2], buf.shape[1], buf.shape[0], 4
    experts, capacity = arrived.shape[0], arrived.shape[1]
    model_width = normed_ref.shape[1]
    tokens = normed_ref.shape[0]
    width = model_width // CHUNKS
    me = (z * x_size + x) * cores + core

    def near(index, step, size):
        return lax.rem(index + step + size, size)

    def member(index):
        return {
            Z: index // (x_size * cores),
            X: lax.rem(index // cores, x_size),
            CORE: lax.rem(index, cores),
        }

    def remote(src, dst, send_sem, recv_sem, peer):
        return pltpu.make_async_remote_copy(
            src_ref=src, dst_ref=dst, send_sem=send_sem, recv_sem=recv_sem,
            device_id=peer, device_id_type=MESH_ID,
        )

    x_right, x_left, x_far = near(x, 1, x_size), near(x, -1, x_size), near(x, 2, x_size)
    right, left = {Y: near(y, 1, y_size)}, {Y: near(y, -1, y_size)}
    barrier = pltpu.get_barrier_semaphore()

    def greet(k, carry):
        pl.semaphore_signal(
            barrier, inc=1, device_id=member(lax.rem(me + k, experts)), device_id_type=MESH_ID
        )
        return carry

    lax.fori_loop(1, experts, greet, 0)
    for peer in (right, left):
        pl.semaphore_signal(barrier, inc=1, device_id=peer, device_id_type=MESH_ID)
    pl.semaphore_wait(barrier, experts + 1)

    def ring_copies(slots, own_source, pick, size, send_sems, recv_sems):
        first, second = pl.ds(0, size // 2), pl.ds(size // 2, size // 2)
        return (
            remote(own_source, pick(slots, 1), send_sems.at[0], recv_sems.at[0], right),
            remote(own_source, pick(slots, 2), send_sems.at[1], recv_sems.at[1], left),
            remote(
                pick(slots, 1, first), pick(slots, 3, first), send_sems.at[2], recv_sems.at[2], right
            ),
            remote(
                pick(slots, 2, second), pick(slots, 3, second), send_sems.at[3], recv_sems.at[3], left
            ),
        )

    def whole(slots, slot, span=None):
        return slots.at[slot] if span is None else slots.at[slot, span]

    depth = gate_ref.shape[0]
    early, late = pl.ds(0, depth // 2), pl.ds(depth // 2, depth // 2)
    gates = (
        remote(gate_ref.at[late], w_gate.at[1, late], w_send.at[0, 0], w_recv.at[0, 0], right),
        remote(gate_ref.at[late], w_gate.at[2, late], w_send.at[0, 1], w_recv.at[0, 1], left),
        remote(gate_left_ref, w_gate.at[3, early], w_send.at[0, 2], w_recv.at[0, 2], right),
        remote(
            w_gate.at[2, late], w_gate.at[3, late], w_send.at[0, 3], w_recv.at[0, 3], left
        ),
    )
    ups = ring_copies(w_up, up_ref, whole, depth, w_send.at[1], w_recv.at[1])
    downs = []
    units = down_ref.shape[0]
    for n in range(CHUNKS):
        columns = pl.ds(n * width, width)

        def some(slots, slot, span=None, columns=columns):
            return slots.at[slot, pl.ds(0, units) if span is None else span, columns]

        downs.append(
            ring_copies(
                w_down, down_ref.at[:, columns], some, units, d_send.at[n], d_recv.at[n]
            )
        )

    def start_both(ring):
        ring[0].start()
        ring[1].start()

    def pass_on(ring):
        ring[0].wait_recv()
        ring[2].start()
        ring[1].wait_recv()
        ring[3].start()

    def far_arrived(ring):
        ring[2].wait_recv()
        ring[3].wait_recv()

    shared = (
        (shared_gate_ref, s_gate, s_gate.shape[1] // (x_size * cores)),
        (shared_up_ref, s_up, s_up.shape[1] // (x_size * cores)),
        (shared_down_ref, s_down, s_down.shape[1] // (x_size * cores)),
    )

    def share(which_x, size, part=None):
        start = (which_x * cores + core) * size
        if part is None:
            return pl.ds(pl.multiple_of(start, size), size)
        return pl.ds(pl.multiple_of(start + part * (size // 2), size // 2), size // 2)

    got = pl.ds(1, 3)
    over_y, over_x, over_cores = [], [], []
    for n, (source, slots, size) in enumerate(shared):
        mine = share(x, size)
        over_y.append((
            remote(source.at[mine], slots.at[1, mine], sy_send.at[n, 0], sy_recv.at[n, 0], right),
            remote(source.at[mine], slots.at[2, mine], sy_send.at[n, 1], sy_recv.at[n, 1], left),
            remote(
                slots.at[1, share(x, size, 0)], slots.at[3, share(x, size, 0)],
                sy_send.at[n, 2], sy_recv.at[n, 2], right,
            ),
            remote(
                slots.at[2, share(x, size, 1)], slots.at[3, share(x, size, 1)],
                sy_send.at[n, 3], sy_recv.at[n, 3], left,
            ),
        ))
        from_left, from_right = share(x_left, size, 0), share(x_right, size, 1)
        over_x.append((
            remote(
                slots.at[got, mine], slots.at[got, mine],
                sx_send.at[n, 0], sx_recv.at[n, 0], {X: x_right},
            ),
            remote(
                slots.at[got, mine], slots.at[got, mine],
                sx_send.at[n, 1], sx_recv.at[n, 1], {X: x_left},
            ),
            remote(
                slots.at[got, from_left], slots.at[got, from_left],
                sx_send.at[n, 2], sx_recv.at[n, 2], {X: x_right},
            ),
            remote(
                slots.at[got, from_right], slots.at[got, from_right],
                sx_send.at[n, 3], sx_recv.at[n, 3], {X: x_left},
            ),
        ))
        over_cores.append([
            remote(
                slots.at[got, share(which, size)], slots.at[got, share(which, size)],
                sc_send.at[n, k], sc_recv.at[n, k], {CORE: 1 - core},
            )
            for k, which in enumerate((x, x_left, x_right, x_far))
        ])

    for ring in over_y:
        start_both(ring)
    gates[2].start()

    blocks = x_size * cores
    relayed = blocks // 2
    z_far, z_below, z_source = near(z, z_size // 2, z_size), near(z, -1, z_size), near(z, 1, z_size)
    relay_target = near(z, -(z_size // 2 - 1), z_size)
    relay_origin = (z_source * x_size + x) * cores + core
    far_blocks = pl.ds(z_far * blocks, relayed)

    def spread(send_one):
        def step(i, carry):
            to = lax.rem(me + lax.rem(i * 13, experts), experts)
            by_relay = jnp.logical_and(to // blocks == z_far, lax.rem(to, blocks) < relayed)

            @pl.when(jnp.logical_not(by_relay))
            def _():
                send_one(to)

            return carry

        lax.fori_loop(1, experts, step, 0)

    row_hop = remote(
        send_ref.at[far_blocks], row_relay, relay_send.at[0], relay_recv.at[0], {Z: z_below}
    )
    row_hop.start()
    along_z = [
        remote(kv_ref, buf.at[core, x, z], z_send.at[k], z_recv.at[k], {Z: near(z, k, z_size)})
        for k in range(1, z_size)
    ]
    for copy in along_z:
        copy.start()
    locals_ = [
        pltpu.make_async_copy(source, target, own_sem.at[n])
        for n, (source, target) in enumerate((
            (kv_ref, buf.at[core, x, z]),
            (send_ref.at[me], arrived.at[me]),
            (gate_ref, w_gate.at[0]),
            (up_ref, w_up.at[0]),
            (down_ref, w_down.at[0]),
            (shared_gate_ref, s_gate.at[0]),
            (shared_up_ref, s_up.at[0]),
            (shared_down_ref, s_down.at[0]),
            (gate_left_ref, w_gate.at[1, early]),
            (gate_right_ref, w_gate.at[2, early]),
        ))
    ]
    for copy in locals_:
        copy.start()
    run_max[...] = jnp.full_like(run_max, -jnp.inf)
    run_sum[...] = jnp.zeros_like(run_sum)
    mixed[...] = jnp.zeros_like(mixed)
    for ring in over_y:
        pass_on(ring)
    start_both(gates)
    start_both(ups)
    locals_[0].wait()
    for copy in along_z:
        copy.wait_recv()
    def attend(which_core, which_x):
        keys = buf.shape[2] * buf.shape[3]

        def tile(i, carry):
            here = pl.ds(i * TILE, TILE)
            span = buf[which_core, which_x].reshape(keys, 128)
            scores = lax.dot_general(
                q_ref[here, :], span, (((1,), (1,)), ((), ())), preferred_element_type=jnp.float32
            )
            old_max = run_max[here, :]
            new_max = jnp.maximum(old_max, jnp.max(scores, axis=1, keepdims=True))
            factor = jnp.exp(old_max - new_max)
            weights_now = jnp.exp(scores - new_max[:, :1])
            run_sum[here, :] = run_sum[here, :] * factor + jnp.sum(
                weights_now, axis=1, keepdims=True
            )
            mixed[here, :] = mixed[here, :] * factor + jnp.dot(
                weights_now.astype(jnp.bfloat16), span, preferred_element_type=jnp.float32
            )
            run_max[here, :] = new_max
            return carry

        lax.fori_loop(0, q_ref.shape[0] // TILE, tile, 0)

    def line_to_core(which_x, slot):
        return remote(
            buf.at[core, which_x], buf.at[core, which_x], c_send.at[slot], c_recv.at[slot],
            {CORE: 1 - core},
        )

    line = buf.at[core, x]
    to_right = remote(line, line, x_send.at[0], x_recv.at[0], {X: x_right})
    to_left = remote(line, line, x_send.at[1], x_recv.at[1], {X: x_left})
    first, second = pl.ds(0, z_size // 2), pl.ds(z_size // 2, z_size // 2)
    on_right = remote(
        buf.at[core, x_left, first], buf.at[core, x_left, first],
        x_send.at[2], x_recv.at[2], {X: x_right},
    )
    on_left = remote(
        buf.at[core, x_right, second], buf.at[core, x_right, second],
        x_send.at[3], x_recv.at[3], {X: x_left},
    )
    lines = [line_to_core(which, n) for n, which in enumerate((x, x_left, x_right, x_far))]
    to_right.start()
    to_left.start()
    lines[0].start()
    spread(
        lambda to: remote(
            send_ref.at[to], arrived.at[me], disp_send, disp_recv, member(to)
        ).start()
    )
    row_hop.wait_recv()

    def relay_row(k, carry):
        remote(
            row_relay.at[k], arrived.at[relay_origin], disp_send, disp_recv,
            member(relay_target * blocks + k),
        ).start()
        return carry

    lax.fori_loop(0, relayed, relay_row, 0)

    attend(core, x)
    lines[0].wait_recv()
    attend(1 - core, x)
    for ring, right_left, lines_now in zip(over_y, over_x, over_cores):
        far_arrived(ring)
        start_both(right_left)
        lines_now[0].start()
    to_right.wait_recv()
    on_right.start()
    lines[1].start()
    to_left.wait_recv()
    on_left.start()
    lines[2].start()
    gates[0].wait_recv()
    gates[1].wait_recv()
    gates[3].start()
    attend(core, x_left)
    attend(core, x_right)
    lines[1].wait_recv()
    attend(1 - core, x_left)
    pass_on(ups)
    start_both(downs[0])
    start_both(downs[1])
    lines[2].wait_recv()
    attend(1 - core, x_right)

    def activated(source, gate_now, up_now):
        gate_proj = jnp.dot(source, gate_now, preferred_element_type=jnp.float32)
        up_proj = jnp.dot(source, up_now, preferred_element_type=jnp.float32)
        return (gate_proj / (1.0 + jnp.exp(-gate_proj)) * up_proj).astype(jnp.bfloat16)

    def shared_part(slot):
        value = activated(normed_ref[...], s_gate[slot], s_up[slot])
        for n in range(CHUNKS):
            columns = slice(n * width, (n + 1) * width)
            product = jnp.dot(value, s_down[slot, :, columns], preferred_element_type=jnp.float32)
            product = product.astype(jnp.bfloat16).astype(jnp.float32)
            if slot == 0:
                shared_sum[:, columns] = product
            else:
                shared_sum[:, columns] += product

    for copy in locals_[1:]:
        copy.wait()
    shared_part(0)

    others = pl.ds(0, experts - 1)
    pltpu.make_async_copy(arrived.at[others], arrived.at[others], disp_recv).wait()

    def flatten(i, carry):
        block = arrived[pl.ds(i * 8, 8)].astype(jnp.float32).reshape(8 * capacity, model_width)
        rows[pl.ds(i * 8 * capacity, 8 * capacity), :] = block.astype(jnp.bfloat16)
        return carry

    lax.fori_loop(0, experts // 8, flatten, 0)

    def fill_hidden(slot):
        def tile(i, carry):
            here = pl.ds(i * TILE, TILE)
            hidden[here, slot * units : (slot + 1) * units] = activated(
                rows[here, :], w_gate[slot], w_up[slot]
            )
            return carry

        lax.fori_loop(0, rows.shape[0] // TILE, tile, 0)

    fill_hidden(0)
    fill_hidden(1)
    fill_hidden(2)
    pass_on(downs[0])
    start_both(downs[2])
    far_arrived(gates)
    far_arrived(ups)
    fill_hidden(3)
    pass_on(downs[1])
    start_both(downs[3])

    def result_hop(n):
        return remote(
            out.at[n, far_blocks], result_relay.at[n],
            relay_send.at[1 + n], relay_recv.at[1 + n], {Z: z_below},
        )

    def relay_results(n):
        result_hop(n).wait_recv()

        def step(k, carry):
            remote(
                result_relay.at[n, k], returned.at[n, relay_origin], ret_send.at[n], ret_recv.at[n],
                member(relay_target * blocks + k),
            ).start()
            return carry

        lax.fori_loop(0, relayed, step, 0)

    for n in range(CHUNKS):
        far_arrived(downs[n])

        def product(i, carry, n=n):
            here = pl.ds(i * TILE, TILE)
            value = jnp.dot(
                hidden[here, :],
                w_down[:, :, n * width : (n + 1) * width].reshape(4 * units, width),
                preferred_element_type=jnp.float32,
            )
            count = TILE // capacity
            out[n, pl.ds(i * count, count)] = value.reshape(count, capacity, width).astype(
                jnp.bfloat16
            )
            return carry

        lax.fori_loop(0, rows.shape[0] // TILE, product, 0)
        result_hop(n).start()
        spread(
            lambda to, n=n: remote(
                out.at[n, to], returned.at[n, me], ret_send.at[n], ret_recv.at[n], member(to)
            ).start()
        )
        pltpu.make_async_copy(out.at[n, me], returned.at[n, me], own_sem.at[10 + n]).start()
        if n + 2 < CHUNKS:
            pass_on(downs[n + 2])
        if n > 0:
            relay_results(n - 1)
        if n == 0:
            for right_left, lines_now in zip(over_x, over_cores):
                pass_on(right_left)
                lines_now[1].start()
                lines_now[2].start()
        if n == 1:
            on_right.wait_recv()
            on_left.wait_recv()
            lines[3].start()
        if n == 2:
            for right_left, lines_now in zip(over_x, over_cores):
                far_arrived(right_left)
                lines_now[3].start()
    attend(core, x_far)
    relay_results(CHUNKS - 1)
    lines[3].wait_recv()
    attend(1 - core, x_far)
    head_rows = attn_ref.shape[0]
    size = 64
    for pair in range(attn_ref.shape[1] // 128):
        heads = []
        for head in (2 * pair, 2 * pair + 1):
            here = slice(head * head_rows, (head + 1) * head_rows)
            heads.append((mixed[here, :] / run_sum[here, :])[:, size:])
        attn_ref[:, pair * 128 : (pair + 1) * 128] = jnp.concatenate(heads, axis=1).astype(
            attn_ref.dtype
        )
    for lines_now in over_cores:
        for copy in lines_now:
            copy.wait_recv()
    for slot in range(1, 4):
        shared_part(slot)

    for n in range(CHUNKS):
        pltpu.make_async_copy(
            returned.at[n, others], returned.at[n, others], ret_recv.at[n]
        ).wait()
        pltpu.make_async_copy(out.at[n, me], returned.at[n, me], own_sem.at[10 + n]).wait()
        columns = slice(n * width, (n + 1) * width)
        results = returned[n].astype(jnp.float32).reshape(experts * capacity, width)
        results = results.astype(jnp.bfloat16)
        total = shared_sum[:, columns]
        routed = None
        for k in range(pick_ref.shape[0]):
            picked = jnp.dot(pick_ref[k], results, preferred_element_type=jnp.float32)
            term = scale_ref[k][:, :1] * picked
            routed = term if routed is None else routed + term
        moe_ref[:, columns] = (routed + total).astype(moe_ref.dtype)

    for ring in [gates, ups] + downs + over_y + over_x + over_cores:
        for copy in ring:
            copy.wait_send()
    for copy in along_z + [to_right, to_left, on_right, on_left, row_hop] + lines:
        copy.wait_send()
    for n in range(CHUNKS):
        result_hop(n).wait_send()
    pltpu.make_async_copy(send_ref.at[others], arrived.at[others], disp_send).wait()
    for n in range(CHUNKS):
        pltpu.make_async_copy(out.at[n, others], returned.at[n, others], ret_send.at[n]).wait()


def run_layer(q_rows, key_value, send, normed, picks, scales, early, expert_weights, shared_weights):
    query_count = q_rows.shape[0]
    tokens = key_value.shape[0]
    z_size, x_size, cores = (lax.axis_size(name) for name in EP)
    experts, capacity, model_width = send.shape
    depth, units = expert_weights[0].shape
    rows, own = experts * capacity, normed.shape[0]
    dma = pltpu.SemaphoreType.DMA
    bf16, f32 = jnp.bfloat16, jnp.float32
    width = model_width // CHUNKS
    vmem, anywhere = pl.BlockSpec(memory_space=pltpu.VMEM), pl.BlockSpec(memory_space=pl.ANY)
    keys = tokens * z_size * x_size * cores
    return pl.pallas_call(
        layer_kernel,
        out_shape=[
            jax.ShapeDtypeStruct((tokens, query_count // tokens * 64), bf16),
            jax.ShapeDtypeStruct(normed.shape, bf16),
        ],
        in_specs=[vmem, vmem, anywhere, vmem, vmem, vmem] + [anywhere] * 8,
        out_specs=[vmem, vmem],
        scratch_shapes=[
            pltpu.VMEM((cores, x_size, z_size, tokens, 128), bf16),
            pltpu.VMEM((query_count, 128), f32),
            pltpu.VMEM((query_count, 128), f32),
            pltpu.VMEM((query_count, 128), f32),
            pltpu.VMEM((4, depth, units), bf16),
            pltpu.VMEM((4, depth, units), bf16),
            pltpu.VMEM((4, units, depth), bf16),
            pltpu.VMEM((4, depth, units), bf16),
            pltpu.VMEM((4, depth, units), bf16),
            pltpu.VMEM((4, units, depth), bf16),
            pltpu.VMEM((experts, capacity, model_width), bf16),
            pltpu.VMEM((rows, model_width), bf16),
            pltpu.VMEM((rows, 4 * units), bf16),
            pltpu.VMEM((CHUNKS, experts, capacity, width), bf16),
            pltpu.VMEM((CHUNKS, experts, capacity, width), bf16),
            pltpu.VMEM((own, model_width), f32),
            pltpu.VMEM((x_size * cores // 2, capacity, model_width), bf16),
            pltpu.VMEM((CHUNKS, x_size * cores // 2, capacity, width), bf16),
            dma((z_size,)), dma((z_size,)),
            dma((4,)), dma((4,)),
            dma((4,)), dma((4,)),
            dma((2, 4)), dma((2, 4)),
            dma((CHUNKS, 4)), dma((CHUNKS, 4)),
            dma, dma,
            dma((CHUNKS,)), dma((CHUNKS,)),
            dma((3, 4)), dma((3, 4)),
            dma((3, 4)), dma((3, 4)),
            dma((3, 4)), dma((3, 4)),
            dma((1 + CHUNKS,)), dma((1 + CHUNKS,)),
            dma((10 + CHUNKS,)),
        ],
        compiler_params=pltpu.CompilerParams(
            collective_id=0, has_side_effects=True, vmem_limit_bytes=60 * 1024 * 1024
        ),
        cost_estimate=pl.CostEstimate(
            flops=60 * query_count * keys * 128 // 2, bytes_accessed=2 * keys * 256, transcendentals=0
        ),
        name="layer",
    )(q_rows, key_value, send, normed, picks, scales, *early, *expert_weights, *shared_weights)


def dispatch(moe_tokens, norm_gain, routes, route_weights):
    tok_rows, model_width = moe_tokens.shape
    top_count = routes.shape[1]
    experts = lax.axis_size(EP)
    capacity = 2 * tok_rows * top_count // experts
    lane = lax.axis_index("tp")
    values32 = moe_tokens.astype(jnp.float32)
    normed = (
        values32
        * lax.rsqrt(jnp.mean(values32 * values32, axis=-1, keepdims=True) + epsilon)
        * norm_gain
    ).astype(jnp.bfloat16)
    own_routes = lax.dynamic_slice_in_dim(routes, lane * tok_rows, tok_rows, 0)
    own_weights = lax.dynamic_slice_in_dim(route_weights, lane * tok_rows, tok_rows, 0)
    gates = own_weights / jnp.sum(own_weights, axis=-1, keepdims=True) * routed_scale
    slots = token_slots(own_routes, capacity)
    places = jnp.arange(experts * capacity, dtype=jnp.int32)
    placed = (places[:, None] == slots[0][None, :]) | (places[:, None] == slots[1][None, :])
    send = jnp.dot(placed.astype(jnp.bfloat16), normed, preferred_element_type=jnp.float32)
    send = send.astype(jnp.bfloat16).reshape(experts, capacity, model_width)
    picks = jnp.stack([(slot[:, None] == places[None, :]).astype(jnp.bfloat16) for slot in slots])
    scales = jnp.broadcast_to(gates.T[:, :, None], (top_count, tok_rows, 128))
    return send, normed, picks, scales


def body(
    query_rows,
    key_rows,
    value_rows,
    query_gain,
    key_gain,
    moe_tokens,
    norm_gain,
    routes,
    route_weights,
    expert_gate,
    expert_up,
    expert_down,
    shared_gate,
    shared_up,
    shared_down,
):
    first_half = expert_gate[0, : expert_gate.shape[1] // 2]
    early = (lax.ppermute(first_half, "tp", ring(1)), lax.ppermute(first_half, "tp", ring(3)))
    dispatched = dispatch(moe_tokens, norm_gain, routes, route_weights)
    row_count = query_rows.shape[0]
    size = query_gain.shape[0]
    heads = query_rows.shape[1] // size
    positions = lax.axis_index(EP) * row_count + jnp.arange(row_count, dtype=jnp.int32)
    q_rot = rotated(query_rows, query_gain, heads, size, positions) * jnp.bfloat16(size**-0.5)
    k_rot = rotated(key_rows, key_gain, 1, size, positions)[0]
    placed = lane_places(1, size, size)[0][0]
    values = jnp.dot(value_rows, placed, preferred_element_type=jnp.float32).astype(jnp.bfloat16)
    attn, moe_out = run_layer(
        q_rot.reshape(heads * row_count, 128),
        k_rot + values,
        *dispatched,
        early,
        (expert_gate[0], expert_up[0], expert_down[0]),
        (shared_gate, shared_up, shared_down),
    )
    return (attn, moe_out)


def solution(mesh):
    finer = Mesh(mesh.devices.reshape(8, 4, 2, mesh.shape["tp"]), ("ep_0", "ep_1", "ep_2", "tp"))
    return jax.shard_map(
        body,
        mesh=finer,
        in_specs=(
            P(EP, "tp"),
            P(EP, "tp"),
            P(EP, "tp"),
            P(),
            P(),
            P(EP_TP, None),
            P(),
            P(EP, None),
            P(EP, None),
            P(EP, None, "tp"),
            P(EP, None, "tp"),
            P(EP, "tp", None),
            P(None, "tp"),
            P(None, "tp"),
            P("tp", None),
        ),
        out_specs=(P(EP, "tp"), P(EP_TP, None)),
        check_vma=False,
    )
```

```python
import functools

import jax
import jax.numpy as jnp
from jax import lax
from jax.experimental import pallas as pl
from jax.experimental.pallas import tpu as pltpu
from jax.sharding import Mesh
from jax.sharding import PartitionSpec as P

GRID_W = 64
EP = ("ep_0", "ep_1", "ep_2")
EP_TP = ("ep_0", "ep_1", "ep_2", "tp")
MESH_ID = pl.DeviceIdType.MESH
Z, X, CORE, Y = EP_TP


epsilon = 1e-06
rotary_base = 10000.0
routed_scale = 2.5


def lane_places(heads, size, offset):
    source = jnp.arange(heads * size)[None, :, None]
    lane = jnp.arange(128)[None, None, :] - offset
    head = jnp.arange(heads)[:, None, None]
    inside = (lane >= 0) & (lane < size)
    straight = inside & (source == head * size + lane)
    swapped = inside & (source == head * size + (lane ^ 1))
    return straight.astype(jnp.bfloat16), swapped.astype(jnp.bfloat16)


def rotated(rows_in, gain, heads, size, positions):
    straight, swapped = lane_places(heads, size, 0)
    own = jnp.einsum("td,hde->hte", rows_in, straight, preferred_element_type=jnp.float32)
    other = jnp.einsum("td,hde->hte", rows_in, swapped, preferred_element_type=jnp.float32)
    lane = jnp.arange(128)
    wide = jnp.pad(gain, (0, 128 - size))
    wide_swapped = jnp.pad(gain.reshape(-1, 2)[:, ::-1].reshape(-1), (0, 128 - size))
    factor = lax.rsqrt(jnp.sum(own * own, axis=-1, keepdims=True) / size + epsilon)
    pair_count = size // 4
    pair = (lane // 2) % (2 * pair_count)
    inv_freq = rotary_base ** (-(pair % pair_count).astype(jnp.float32) / pair_count)
    grid_row = (positions // GRID_W).astype(jnp.float32)[:, None]
    grid_col = (positions % GRID_W).astype(jnp.float32)[:, None]
    angles = jnp.where(pair[None, :] < pair_count, grid_row, grid_col) * inv_freq[None, :]
    sign = jnp.where(lane % 2 == 0, -1.0, 1.0)
    turned = (own * factor * wide) * jnp.cos(angles) + (other * factor * wide_swapped) * (
        sign * jnp.sin(angles)
    )
    return turned.astype(jnp.bfloat16)


def ring(step):
    return [(i, (i + step) % 4) for i in range(4)]


def token_slots(own_routes, capacity):
    rows = own_routes.shape[0]
    earlier = jnp.arange(rows)[:, None] < jnp.arange(rows)[None, :]
    slots = []
    for k in range(own_routes.shape[1]):
        mine = own_routes[:, k]
        same = own_routes[:, 0][:, None] == mine[None, :]
        for other in range(1, own_routes.shape[1]):
            same = same | (own_routes[:, other][:, None] == mine[None, :])
        rank = jnp.sum((same & earlier).astype(jnp.int32), axis=0)
        slots.append(mine * capacity + rank)
    return slots


CHUNKS = 4
TILE = 256


def layer_kernel(
    q_ref, kv_ref, send_ref, normed_ref, pick_ref, scale_ref,
    gate_left_ref, gate_right_ref,
    gate_ref, up_ref, down_ref, shared_gate_ref, shared_up_ref, shared_down_ref,
    attn_ref, moe_ref,
    buf, run_max, run_sum, mixed,
    w_gate, w_up, w_down, s_gate, s_up, s_down,
    arrived, rows, hidden, out, returned,
    shared_sum, row_relay, result_relay,
    z_send, z_recv, x_send, x_recv, c_send, c_recv, w_send, w_recv, d_send, d_recv,
    disp_send, disp_recv, ret_send, ret_recv, sy_send, sy_recv, sx_send, sx_recv, sc_send, sc_recv,
    relay_send, relay_recv, own_sem,
):
    z, x, core, y = (lax.axis_index(name) for name in EP_TP)
    z_size, x_size, cores, y_size = buf.shape[2], buf.shape[1], buf.shape[0], 4
    experts, capacity = arrived.shape[0], arrived.shape[1]
    model_width = normed_ref.shape[1]
    tokens = normed_ref.shape[0]
    width = model_width // CHUNKS
    me = (z * x_size + x) * cores + core

    def near(index, step, size):
        return lax.rem(index + step + size, size)

    def member(index):
        return {
            Z: index // (x_size * cores),
            X: lax.rem(index // cores, x_size),
            CORE: lax.rem(index, cores),
        }

    def remote(src, dst, send_sem, recv_sem, peer):
        return pltpu.make_async_remote_copy(
            src_ref=src, dst_ref=dst, send_sem=send_sem, recv_sem=recv_sem,
            device_id=peer, device_id_type=MESH_ID,
        )

    x_right, x_left, x_far = near(x, 1, x_size), near(x, -1, x_size), near(x, 2, x_size)
    right, left = {Y: near(y, 1, y_size)}, {Y: near(y, -1, y_size)}
    barrier = pltpu.get_barrier_semaphore()

    def greet(k, carry):
        pl.semaphore_signal(
            barrier, inc=1, device_id=member(lax.rem(me + k, experts)), device_id_type=MESH_ID
        )
        return carry

    lax.fori_loop(1, experts, greet, 0)
    for peer in (right, left):
        pl.semaphore_signal(barrier, inc=1, device_id=peer, device_id_type=MESH_ID)
    pl.semaphore_wait(barrier, experts + 1)

    def ring_copies(slots, own_source, pick, size, send_sems, recv_sems):
        first, second = pl.ds(0, size // 2), pl.ds(size // 2, size // 2)
        return (
            remote(own_source, pick(slots, 1), send_sems.at[0], recv_sems.at[0], right),
            remote(own_source, pick(slots, 2), send_sems.at[1], recv_sems.at[1], left),
            remote(
                pick(slots, 1, first), pick(slots, 3, first), send_sems.at[2], recv_sems.at[2], right
            ),
            remote(
                pick(slots, 2, second), pick(slots, 3, second), send_sems.at[3], recv_sems.at[3], left
            ),
        )

    def whole(slots, slot, span=None):
        return slots.at[slot] if span is None else slots.at[slot, span]

    depth = gate_ref.shape[0]
    early, late = pl.ds(0, depth // 2), pl.ds(depth // 2, depth // 2)
    gates = (
        remote(gate_ref.at[late], w_gate.at[1, late], w_send.at[0, 0], w_recv.at[0, 0], right),
        remote(gate_ref.at[late], w_gate.at[2, late], w_send.at[0, 1], w_recv.at[0, 1], left),
        remote(gate_left_ref, w_gate.at[3, early], w_send.at[0, 2], w_recv.at[0, 2], right),
        remote(
            w_gate.at[2, late], w_gate.at[3, late], w_send.at[0, 3], w_recv.at[0, 3], left
        ),
    )
    ups = ring_copies(w_up, up_ref, whole, depth, w_send.at[1], w_recv.at[1])
    downs = []
    units = down_ref.shape[0]
    for n in range(CHUNKS):
        columns = pl.ds(n * width, width)

        def some(slots, slot, span=None, columns=columns):
            return slots.at[slot, pl.ds(0, units) if span is None else span, columns]

        downs.append(
            ring_copies(
                w_down, down_ref.at[:, columns], some, units, d_send.at[n], d_recv.at[n]
            )
        )

    def start_both(ring):
        ring[0].start()
        ring[1].start()

    def pass_on(ring):
        ring[0].wait_recv()
        ring[2].start()
        ring[1].wait_recv()
        ring[3].start()

    def far_arrived(ring):
        ring[2].wait_recv()
        ring[3].wait_recv()

    shared = (
        (shared_gate_ref, s_gate, s_gate.shape[1] // (x_size * cores)),
        (shared_up_ref, s_up, s_up.shape[1] // (x_size * cores)),
        (shared_down_ref, s_down, s_down.shape[1] // (x_size * cores)),
    )

    def share(which_x, size, part=None):
        start = (which_x * cores + core) * size
        if part is None:
            return pl.ds(pl.multiple_of(start, size), size)
        return pl.ds(pl.multiple_of(start + part * (size // 2), size // 2), size // 2)

    got = pl.ds(1, 3)
    over_y, over_x, over_cores = [], [], []
    for n, (source, slots, size) in enumerate(shared):
        mine = share(x, size)
        over_y.append((
            remote(source.at[mine], slots.at[1, mine], sy_send.at[n, 0], sy_recv.at[n, 0], right),
            remote(source.at[mine], slots.at[2, mine], sy_send.at[n, 1], sy_recv.at[n, 1], left),
            remote(
                slots.at[1, share(x, size, 0)], slots.at[3, share(x, size, 0)],
                sy_send.at[n, 2], sy_recv.at[n, 2], right,
            ),
            remote(
                slots.at[2, share(x, size, 1)], slots.at[3, share(x, size, 1)],
                sy_send.at[n, 3], sy_recv.at[n, 3], left,
            ),
        ))
        from_left, from_right = share(x_left, size, 0), share(x_right, size, 1)
        over_x.append((
            remote(
                slots.at[got, mine], slots.at[got, mine],
                sx_send.at[n, 0], sx_recv.at[n, 0], {X: x_right},
            ),
            remote(
                slots.at[got, mine], slots.at[got, mine],
                sx_send.at[n, 1], sx_recv.at[n, 1], {X: x_left},
            ),
            remote(
                slots.at[got, from_left], slots.at[got, from_left],
                sx_send.at[n, 2], sx_recv.at[n, 2], {X: x_right},
            ),
            remote(
                slots.at[got, from_right], slots.at[got, from_right],
                sx_send.at[n, 3], sx_recv.at[n, 3], {X: x_left},
            ),
        ))
        over_cores.append([
            remote(
                slots.at[got, share(which, size)], slots.at[got, share(which, size)],
                sc_send.at[n, k], sc_recv.at[n, k], {CORE: 1 - core},
            )
            for k, which in enumerate((x, x_left, x_right, x_far))
        ])

    for ring in over_y:
        start_both(ring)
    gates[2].start()

    blocks = x_size * cores
    relayed = blocks // 2
    z_far, z_below, z_source = near(z, z_size // 2, z_size), near(z, -1, z_size), near(z, 1, z_size)
    relay_target = near(z, -(z_size // 2 - 1), z_size)
    relay_origin = (z_source * x_size + x) * cores + core
    far_blocks = pl.ds(z_far * blocks, relayed)

    def spread(send_one):
        def step(i, carry):
            to = lax.rem(me + lax.rem(i * 13, experts), experts)
            by_relay = jnp.logical_and(to // blocks == z_far, lax.rem(to, blocks) < relayed)

            @pl.when(jnp.logical_not(by_relay))
            def _():
                send_one(to)

            return carry

        lax.fori_loop(1, experts, step, 0)

    row_hop = remote(
        send_ref.at[far_blocks], row_relay, relay_send.at[0], relay_recv.at[0], {Z: z_below}
    )
    row_hop.start()
    along_z = [
        remote(kv_ref, buf.at[core, x, z], z_send.at[k], z_recv.at[k], {Z: near(z, k, z_size)})
        for k in range(1, z_size)
    ]
    for copy in along_z:
        copy.start()
    locals_ = [
        pltpu.make_async_copy(source, target, own_sem.at[n])
        for n, (source, target) in enumerate((
            (kv_ref, buf.at[core, x, z]),
            (send_ref.at[me], arrived.at[me]),
            (gate_ref, w_gate.at[0]),
            (up_ref, w_up.at[0]),
            (down_ref, w_down.at[0]),
            (shared_gate_ref, s_gate.at[0]),
            (shared_up_ref, s_up.at[0]),
            (shared_down_ref, s_down.at[0]),
            (gate_left_ref, w_gate.at[1, early]),
            (gate_right_ref, w_gate.at[2, early]),
        ))
    ]
    for copy in locals_:
        copy.start()
    run_max[...] = jnp.full_like(run_max, -jnp.inf)
    run_sum[...] = jnp.zeros_like(run_sum)
    mixed[...] = jnp.zeros_like(mixed)
    for ring in over_y:
        pass_on(ring)
    start_both(gates)
    start_both(ups)
    locals_[0].wait()
    for copy in along_z:
        copy.wait_recv()
    def attend(which_core, which_x):
        keys = buf.shape[2] * buf.shape[3]

        def tile(i, carry):
            here = pl.ds(i * TILE, TILE)
            span = buf[which_core, which_x].reshape(keys, 128)
            scores = lax.dot_general(
                q_ref[here, :], span, (((1,), (1,)), ((), ())), preferred_element_type=jnp.float32
            )
            old_max = run_max[here, :]
            new_max = jnp.maximum(old_max, jnp.max(scores, axis=1, keepdims=True))
            factor = jnp.exp(old_max - new_max)
            weights_now = jnp.exp(scores - new_max[:, :1])
            run_sum[here, :] = run_sum[here, :] * factor + jnp.sum(
                weights_now, axis=1, keepdims=True
            )
            mixed[here, :] = mixed[here, :] * factor + jnp.dot(
                weights_now.astype(jnp.bfloat16), span, preferred_element_type=jnp.float32
            )
            run_max[here, :] = new_max
            return carry

        lax.fori_loop(0, q_ref.shape[0] // TILE, tile, 0)

    def line_to_core(which_x, slot):
        return remote(
            buf.at[core, which_x], buf.at[core, which_x], c_send.at[slot], c_recv.at[slot],
            {CORE: 1 - core},
        )

    line = buf.at[core, x]
    to_right = remote(line, line, x_send.at[0], x_recv.at[0], {X: x_right})
    to_left = remote(line, line, x_send.at[1], x_recv.at[1], {X: x_left})
    first, second = pl.ds(0, z_size // 2), pl.ds(z_size // 2, z_size // 2)
    on_right = remote(
        buf.at[core, x_left, first], buf.at[core, x_left, first],
        x_send.at[2], x_recv.at[2], {X: x_right},
    )
    on_left = remote(
        buf.at[core, x_right, second], buf.at[core, x_right, second],
        x_send.at[3], x_recv.at[3], {X: x_left},
    )
    lines = [line_to_core(which, n) for n, which in enumerate((x, x_left, x_right, x_far))]
    to_right.start()
    to_left.start()
    lines[0].start()
    spread(
        lambda to: remote(
            send_ref.at[to], arrived.at[me], disp_send, disp_recv, member(to)
        ).start()
    )
    row_hop.wait_recv()

    def relay_row(k, carry):
        remote(
            row_relay.at[k], arrived.at[relay_origin], disp_send, disp_recv,
            member(relay_target * blocks + k),
        ).start()
        return carry

    lax.fori_loop(0, relayed, relay_row, 0)

    attend(core, x)
    lines[0].wait_recv()
    attend(1 - core, x)
    for ring, right_left, lines_now in zip(over_y, over_x, over_cores):
        far_arrived(ring)
        start_both(right_left)
        lines_now[0].start()
    to_right.wait_recv()
    on_right.start()
    lines[1].start()
    to_left.wait_recv()
    on_left.start()
    lines[2].start()
    gates[0].wait_recv()
    gates[1].wait_recv()
    gates[3].start()
    attend(core, x_left)
    attend(core, x_right)
    lines[1].wait_recv()
    attend(1 - core, x_left)
    pass_on(ups)
    start_both(downs[0])
    lines[2].wait_recv()
    attend(1 - core, x_right)

    def activated(source, gate_now, up_now):
        gate_proj = jnp.dot(source, gate_now, preferred_element_type=jnp.float32)
        up_proj = jnp.dot(source, up_now, preferred_element_type=jnp.float32)
        return (gate_proj / (1.0 + jnp.exp(-gate_proj)) * up_proj).astype(jnp.bfloat16)

    def shared_part(slot):
        value = activated(normed_ref[...], s_gate[slot], s_up[slot])
        for n in range(CHUNKS):
            columns = slice(n * width, (n + 1) * width)
            product = jnp.dot(value, s_down[slot, :, columns], preferred_element_type=jnp.float32)
            product = product.astype(jnp.bfloat16).astype(jnp.float32)
            if slot == 0:
                shared_sum[:, columns] = product
            else:
                shared_sum[:, columns] += product

    for copy in locals_[1:]:
        copy.wait()
    shared_part(0)

    others = pl.ds(0, experts - 1)
    pltpu.make_async_copy(arrived.at[others], arrived.at[others], disp_recv).wait()

    def flatten(i, carry):
        block = arrived[pl.ds(i * 8, 8)].astype(jnp.float32).reshape(8 * capacity, model_width)
        rows[pl.ds(i * 8 * capacity, 8 * capacity), :] = block.astype(jnp.bfloat16)
        return carry

    lax.fori_loop(0, experts // 8, flatten, 0)

    def fill_hidden(slot):
        def tile(i, carry):
            here = pl.ds(i * TILE, TILE)
            hidden[here, slot * units : (slot + 1) * units] = activated(
                rows[here, :], w_gate[slot], w_up[slot]
            )
            return carry

        lax.fori_loop(0, rows.shape[0] // TILE, tile, 0)

    fill_hidden(0)
    fill_hidden(1)
    fill_hidden(2)
    pass_on(downs[0])
    start_both(downs[1])
    far_arrived(gates)
    far_arrived(ups)
    fill_hidden(3)

    def result_hop(n):
        return remote(
            out.at[n, far_blocks], result_relay.at[n],
            relay_send.at[1 + n], relay_recv.at[1 + n], {Z: z_below},
        )

    def relay_results(n):
        result_hop(n).wait_recv()

        def step(k, carry):
            remote(
                result_relay.at[n, k], returned.at[n, relay_origin], ret_send.at[n], ret_recv.at[n],
                member(relay_target * blocks + k),
            ).start()
            return carry

        lax.fori_loop(0, relayed, step, 0)

    for n in range(CHUNKS):
        far_arrived(downs[n])

        def product(i, carry, n=n):
            here = pl.ds(i * TILE, TILE)
            value = jnp.dot(
                hidden[here, :],
                w_down[:, :, n * width : (n + 1) * width].reshape(4 * units, width),
                preferred_element_type=jnp.float32,
            )
            count = TILE // capacity
            out[n, pl.ds(i * count, count)] = value.reshape(count, capacity, width).astype(
                jnp.bfloat16
            )
            return carry

        lax.fori_loop(0, rows.shape[0] // TILE, product, 0)
        result_hop(n).start()
        spread(
            lambda to, n=n: remote(
                out.at[n, to], returned.at[n, me], ret_send.at[n], ret_recv.at[n], member(to)
            ).start()
        )
        pltpu.make_async_copy(out.at[n, me], returned.at[n, me], own_sem.at[10 + n]).start()
        if n + 1 < CHUNKS:
            pass_on(downs[n + 1])
        if n + 2 < CHUNKS:
            start_both(downs[n + 2])
        if n > 0:
            relay_results(n - 1)
        if n == 0:
            for right_left, lines_now in zip(over_x, over_cores):
                pass_on(right_left)
                lines_now[1].start()
                lines_now[2].start()
        if n == 1:
            on_right.wait_recv()
            on_left.wait_recv()
            lines[3].start()
        if n == 2:
            for right_left, lines_now in zip(over_x, over_cores):
                far_arrived(right_left)
                lines_now[3].start()
    attend(core, x_far)
    relay_results(CHUNKS - 1)
    lines[3].wait_recv()
    attend(1 - core, x_far)
    head_rows = attn_ref.shape[0]
    size = 64
    for pair in range(attn_ref.shape[1] // 128):
        heads = []
        for head in (2 * pair, 2 * pair + 1):
            here = slice(head * head_rows, (head + 1) * head_rows)
            heads.append((mixed[here, :] / run_sum[here, :])[:, size:])
        attn_ref[:, pair * 128 : (pair + 1) * 128] = jnp.concatenate(heads, axis=1).astype(
            attn_ref.dtype
        )
    for lines_now in over_cores:
        for copy in lines_now:
            copy.wait_recv()
    for slot in range(1, 4):
        shared_part(slot)

    for n in range(CHUNKS):
        pltpu.make_async_copy(
            returned.at[n, others], returned.at[n, others], ret_recv.at[n]
        ).wait()
        pltpu.make_async_copy(out.at[n, me], returned.at[n, me], own_sem.at[10 + n]).wait()
        columns = slice(n * width, (n + 1) * width)
        results = returned[n].astype(jnp.float32).reshape(experts * capacity, width)
        results = results.astype(jnp.bfloat16)
        total = shared_sum[:, columns]
        routed = None
        for k in range(pick_ref.shape[0]):
            picked = jnp.dot(pick_ref[k], results, preferred_element_type=jnp.float32)
            term = scale_ref[k][:, :1] * picked
            routed = term if routed is None else routed + term
        moe_ref[:, columns] = (routed + total).astype(moe_ref.dtype)

    for ring in [gates, ups] + downs + over_y + over_x + over_cores:
        for copy in ring:
            copy.wait_send()
    for copy in along_z + [to_right, to_left, on_right, on_left, row_hop] + lines:
        copy.wait_send()
    for n in range(CHUNKS):
        result_hop(n).wait_send()
    pltpu.make_async_copy(send_ref.at[others], arrived.at[others], disp_send).wait()
    for n in range(CHUNKS):
        pltpu.make_async_copy(out.at[n, others], returned.at[n, others], ret_send.at[n]).wait()


def run_layer(q_rows, key_value, send, normed, picks, scales, early, expert_weights, shared_weights):
    query_count = q_rows.shape[0]
    tokens = key_value.shape[0]
    z_size, x_size, cores = (lax.axis_size(name) for name in EP)
    experts, capacity, model_width = send.shape
    depth, units = expert_weights[0].shape
    rows, own = experts * capacity, normed.shape[0]
    dma = pltpu.SemaphoreType.DMA
    bf16, f32 = jnp.bfloat16, jnp.float32
    width = model_width // CHUNKS
    vmem, anywhere = pl.BlockSpec(memory_space=pltpu.VMEM), pl.BlockSpec(memory_space=pl.ANY)
    keys = tokens * z_size * x_size * cores
    return pl.pallas_call(
        layer_kernel,
        out_shape=[
            jax.ShapeDtypeStruct((tokens, query_count // tokens * 64), bf16),
            jax.ShapeDtypeStruct(normed.shape, bf16),
        ],
        in_specs=[vmem, vmem, anywhere, vmem, vmem, vmem] + [anywhere] * 8,
        out_specs=[vmem, vmem],
        scratch_shapes=[
            pltpu.VMEM((cores, x_size, z_size, tokens, 128), bf16),
            pltpu.VMEM((query_count, 128), f32),
            pltpu.VMEM((query_count, 128), f32),
            pltpu.VMEM((query_count, 128), f32),
            pltpu.VMEM((4, depth, units), bf16),
            pltpu.VMEM((4, depth, units), bf16),
            pltpu.VMEM((4, units, depth), bf16),
            pltpu.VMEM((4, depth, units), bf16),
            pltpu.VMEM((4, depth, units), bf16),
            pltpu.VMEM((4, units, depth), bf16),
            pltpu.VMEM((experts, capacity, model_width), bf16),
            pltpu.VMEM((rows, model_width), bf16),
            pltpu.VMEM((rows, 4 * units), bf16),
            pltpu.VMEM((CHUNKS, experts, capacity, width), bf16),
            pltpu.VMEM((CHUNKS, experts, capacity, width), bf16),
            pltpu.VMEM((own, model_width), f32),
            pltpu.VMEM((x_size * cores // 2, capacity, model_width), bf16),
            pltpu.VMEM((CHUNKS, x_size * cores // 2, capacity, width), bf16),
            dma((z_size,)), dma((z_size,)),
            dma((4,)), dma((4,)),
            dma((4,)), dma((4,)),
            dma((2, 4)), dma((2, 4)),
            dma((CHUNKS, 4)), dma((CHUNKS, 4)),
            dma, dma,
            dma((CHUNKS,)), dma((CHUNKS,)),
            dma((3, 4)), dma((3, 4)),
            dma((3, 4)), dma((3, 4)),
            dma((3, 4)), dma((3, 4)),
            dma((1 + CHUNKS,)), dma((1 + CHUNKS,)),
            dma((10 + CHUNKS,)),
        ],
        compiler_params=pltpu.CompilerParams(
            collective_id=0, has_side_effects=True, vmem_limit_bytes=60 * 1024 * 1024
        ),
        cost_estimate=pl.CostEstimate(
            flops=60 * query_count * keys * 128 // 2, bytes_accessed=2 * keys * 256, transcendentals=0
        ),
        name="layer",
    )(q_rows, key_value, send, normed, picks, scales, *early, *expert_weights, *shared_weights)


def dispatch(moe_tokens, norm_gain, routes, route_weights):
    tok_rows, model_width = moe_tokens.shape
    top_count = routes.shape[1]
    experts = lax.axis_size(EP)
    capacity = 2 * tok_rows * top_count // experts
    lane = lax.axis_index("tp")
    values32 = moe_tokens.astype(jnp.float32)
    normed = (
        values32
        * lax.rsqrt(jnp.mean(values32 * values32, axis=-1, keepdims=True) + epsilon)
        * norm_gain
    ).astype(jnp.bfloat16)
    own_routes = lax.dynamic_slice_in_dim(routes, lane * tok_rows, tok_rows, 0)
    own_weights = lax.dynamic_slice_in_dim(route_weights, lane * tok_rows, tok_rows, 0)
    gates = own_weights / jnp.sum(own_weights, axis=-1, keepdims=True) * routed_scale
    slots = token_slots(own_routes, capacity)
    places = jnp.arange(experts * capacity, dtype=jnp.int32)
    placed = (places[:, None] == slots[0][None, :]) | (places[:, None] == slots[1][None, :])
    send = jnp.dot(placed.astype(jnp.bfloat16), normed, preferred_element_type=jnp.float32)
    send = send.astype(jnp.bfloat16).reshape(experts, capacity, model_width)
    picks = jnp.stack([(slot[:, None] == places[None, :]).astype(jnp.bfloat16) for slot in slots])
    scales = jnp.broadcast_to(gates.T[:, :, None], (top_count, tok_rows, 128))
    return send, normed, picks, scales


def body(
    query_rows,
    key_rows,
    value_rows,
    query_gain,
    key_gain,
    moe_tokens,
    norm_gain,
    routes,
    route_weights,
    expert_gate,
    expert_up,
    expert_down,
    shared_gate,
    shared_up,
    shared_down,
):
    first_half = expert_gate[0, : expert_gate.shape[1] // 2]
    early = (lax.ppermute(first_half, "tp", ring(1)), lax.ppermute(first_half, "tp", ring(3)))
    dispatched = dispatch(moe_tokens, norm_gain, routes, route_weights)
    row_count = query_rows.shape[0]
    size = query_gain.shape[0]
    heads = query_rows.shape[1] // size
    positions = lax.axis_index(EP) * row_count + jnp.arange(row_count, dtype=jnp.int32)
    q_rot = rotated(query_rows, query_gain, heads, size, positions) * jnp.bfloat16(size**-0.5)
    k_rot = rotated(key_rows, key_gain, 1, size, positions)[0]
    placed = lane_places(1, size, size)[0][0]
    values = jnp.dot(value_rows, placed, preferred_element_type=jnp.float32).astype(jnp.bfloat16)
    attn, moe_out = run_layer(
        q_rot.reshape(heads * row_count, 128),
        k_rot + values,
        *dispatched,
        early,
        (expert_gate[0], expert_up[0], expert_down[0]),
        (shared_gate, shared_up, shared_down),
    )
    return (attn, moe_out)


def solution(mesh):
    finer = Mesh(mesh.devices.reshape(8, 4, 2, mesh.shape["tp"]), ("ep_0", "ep_1", "ep_2", "tp"))
    return jax.shard_map(
        body,
        mesh=finer,
        in_specs=(
            P(EP, "tp"),
            P(EP, "tp"),
            P(EP, "tp"),
            P(),
            P(),
            P(EP_TP, None),
            P(),
            P(EP, None),
            P(EP, None),
            P(EP, None, "tp"),
            P(EP, None, "tp"),
            P(EP, "tp", None),
            P(None, "tp"),
            P(None, "tp"),
            P("tp", None),
        ),
        out_specs=(P(EP, "tp"), P(EP_TP, None)),
        check_vma=False,
    )
```
